128 devices in a mesh: rep: 2 (over z_hi), fs: 32 (over z_lo, y, x), tp: 2 (over core).
Axes of the slice: x: 4, y: 4, z: 4 (z_hi: 2, z_lo: 2; z = z_hi * 2 + z_lo), core: 2. Of those that a mesh axis runs over, the one named last changes fastest.
Arguments:
- tokens: bfloat16 [32768, 2048], P(('rep', 'fs'), 'tp'), may hold values from -6 to 6
- mix_gain: float32 [2048], replicated, may hold values from 0.1 to 1.9
- lru_input: float32 [2048, 2048], P('fs', 'tp'), may hold values from -0.125 to 0.125
- lru_gate: float32 [2048, 2048], P('fs', 'tp'), may hold values from -0.125 to 0.125
- lru_input_scale: float32 [2048], P('tp'), may hold values from 0.5 to 2
- lru_gate_scale: float32 [2048], P('tp'), may hold values from 0.5 to 2
- conv_weight: float32 [4, 2048], P(None, 'tp'), may hold values from -3 to 3
- recur_gate: float32 [32, 64, 64], P('tp'), may hold values from -0.75 to 0.75
- input_gate: float32 [32, 64, 64], P('tp'), may hold values from -0.75 to 0.75
- decay_rate: float32 [2048], P('tp'), may hold values from 3.5 to 9
- extra_decay: float32 [32768], P(('rep', 'fs')), may hold values from 0.0003 to 2.1
- lru_output: float32 [2048, 2048], P('tp', 'fs'), may hold values from -0.125 to 0.125
- lru_output_scale: float32 [2048], replicated, may hold values from 0.5 to 2
- ffn_gain: float32 [2048], replicated, may hold values from 0.1 to 1.9
- ffn_gate: float32 [2048, 2816], P('fs', 'tp'), may hold values from -0.125 to 0.125
- ffn_up: float32 [2048, 2816], P('fs', 'tp'), may hold values from -0.125 to 0.125
- ffn_gate_scale: float32 [2816], P('tp'), may hold values from 0.5 to 2
- ffn_up_scale: float32 [2816], P('tp'), may hold values from 0.5 to 2
- ffn_down: float32 [2816, 2048], P('tp', 'fs'), may hold values from -0.109375 to 0.109375
- ffn_down_scale: float32 [2048], replicated, may hold values from 0.5 to 2
Outputs:
- layer_out: bfloat16 [32768, 2048], P(('rep', 'fs'), 'tp')
The draws below stay inside these ranges and needn't reach their ends.
All inputs are finite; a program needn't handle non-finite values.
Results may differ from the reference program's by a relative error of at most 0.02.
Values may be sent and summed in bfloat16 or wider, within the bound.
A program may use at most 192 MiB of HBM per device.

```python
import math
import jax
import jax.numpy as jnp
from jax import lax

D = 2048
FF = 2816
BDIM = 64
LRU_BLOCKS = 32
CONV = 4
TOK_DEV = 512
LRU = 2048
SEQS = 64
TOKENS = 32768
N_TP = 2


def draw_decay_rate(key, part):
    first, second, third = jax.random.split(jax.random.fold_in(key, 11), 3)
    share = 0.5
    slow = jax.random.uniform(first, (LRU,), jnp.float32) < share
    slow_value = jax.random.uniform(second, (LRU,), jnp.float32, 8.0, 9.0)
    fast_value = jax.random.uniform(third, (LRU,), jnp.float32, 3.5, 4.5)
    return jnp.where(slow, slow_value, fast_value)


def draw_extra_decay(key, part):
    first, second, third = jax.random.split(jax.random.fold_in(key, 23), 3)
    base = jnp.exp(jax.random.uniform(first, (SEQS, 1), jnp.float32, jnp.log(0.0003), jnp.log(0.0009)))
    spots = jax.random.randint(second, (SEQS, 3), 0, TOK_DEV)
    where = jnp.arange(TOK_DEV, dtype=jnp.int32)
    hits = jnp.sum((where[None, None, :] == spots[:, :, None]).astype(jnp.float32), axis=1)
    sizes = jax.random.uniform(third, (SEQS, TOK_DEV), jnp.float32, 0.22, 0.69)
    return (base + hits * sizes).reshape(TOKENS)


def block_scale(rng, shape, cuts, smallest, top_value):
    def one(position, shards_of):
        draws = jax.random.uniform(jax.random.fold_in(jax.random.fold_in(rng, 6), position), (shards_of,), jnp.float32, smallest / len(cuts), top_value / len(cuts))
        return jnp.repeat(jnp.exp(draws), shape[position] // shards_of).reshape((-1,) + (1,) * (len(shape) - position - 1))

    loudness = one(*cuts[0])
    for cut in cuts[1:]:
        loudness = loudness * one(*cut)
    return loudness


def gaussian(rng, shape, scale, most, cuts=(), kind=jnp.bfloat16):
    entries = jax.random.normal(rng, shape, jnp.float32) * scale
    if len(cuts) > 0:
        entries = block_scale(rng, shape, cuts, -0.22, 0.18) * entries
    return jnp.clip(entries, min=-most, max=most).astype(kind)


def setup_inputs(seed: int = 0) -> dict:
    key_of = jax.random.split(jax.random.key(seed), 21)
    tokens = gaussian(key_of[0], (TOKENS, D), 1.0, 6.0, ((0, 64), (1, 2)))
    mix_gain = jnp.clip(1.0 + 0.18 * jax.random.normal(key_of[1], (D,), jnp.float32), 0.1, 1.9)
    lru_input = gaussian(key_of[2], (D, LRU), D ** -0.5, 0.125, ((0, 32), (1, 2)), jnp.float32)
    lru_gate = gaussian(key_of[3], (D, LRU), D ** -0.5, 0.125, ((0, 32), (1, 2)), jnp.float32)
    lru_input_scale = jnp.clip(jnp.exp(math.log(2.0) - 1.3862944 * jax.random.uniform(key_of[4], (LRU,), jnp.float32) ** block_scale(key_of[4], (LRU,), ((0, 2),), -0.2, 0.2)), 0.5, 2.0)
    lru_gate_scale = jnp.clip(jnp.exp(math.log(2.0) - 1.3862944 * jax.random.uniform(key_of[5], (LRU,), jnp.float32) ** block_scale(key_of[5], (LRU,), ((0, 2),), -0.2, 0.2)), 0.5, 2.0)
    conv_weight = gaussian(key_of[6], (CONV, LRU), 0.5, 3.0, ((1, 2),), jnp.float32)
    recur_gate = gaussian(key_of[7], (LRU_BLOCKS, BDIM, BDIM), BDIM ** -0.5, 0.75, ((0, 2),), jnp.float32)
    input_gate = gaussian(key_of[8], (LRU_BLOCKS, BDIM, BDIM), BDIM ** -0.5, 0.75, ((0, 2),), jnp.float32)
    decay_rate = draw_decay_rate(jax.random.fold_in(key_of[20], 71), 0)
    extra_decay = draw_extra_decay(jax.random.fold_in(key_of[20], 71), 0)
    lru_output = gaussian(key_of[11], (LRU, D), LRU ** -0.5, 0.125, ((0, 2), (1, 32)), jnp.float32)
    lru_output_scale = jnp.clip(jnp.exp(jax.random.uniform(key_of[12], (D,), jnp.float32, math.log(0.5), math.log(2.0))), 0.5, 2.0)
    ffn_gain = jnp.clip(1.0 + 0.18 * jax.random.normal(key_of[13], (D,), jnp.float32), 0.1, 1.9)
    ffn_gate = gaussian(key_of[14], (D, FF), D ** -0.5, 0.125, ((0, 32), (1, 2)), jnp.float32)
    ffn_up = gaussian(key_of[15], (D, FF), D ** -0.5, 0.125, ((0, 32), (1, 2)), jnp.float32)
    ffn_gate_scale = jnp.clip(jnp.exp(math.log(2.0) - 1.3862944 * jax.random.uniform(key_of[16], (FF,), jnp.float32) ** block_scale(key_of[16], (FF,), ((0, 2),), -0.2, 0.2)), 0.5, 2.0)
    ffn_up_scale = jnp.clip(jnp.exp(math.log(2.0) - 1.3862944 * jax.random.uniform(key_of[17], (FF,), jnp.float32) ** block_scale(key_of[17], (FF,), ((0, 2),), -0.2, 0.2)), 0.5, 2.0)
    ffn_down = gaussian(key_of[18], (FF, D), FF ** -0.5, 0.109375, ((0, 2), (1, 32)), jnp.float32)
    ffn_down_scale = jnp.clip(jnp.exp(jax.random.uniform(key_of[19], (D,), jnp.float32, math.log(0.5), math.log(2.0))), 0.5, 2.0)
    return dict(tokens=tokens, mix_gain=mix_gain, lru_input=lru_input, lru_gate=lru_gate, lru_input_scale=lru_input_scale, lru_gate_scale=lru_gate_scale, conv_weight=conv_weight, recur_gate=recur_gate, input_gate=input_gate, decay_rate=decay_rate, extra_decay=extra_decay, lru_output=lru_output, lru_output_scale=lru_output_scale, ffn_gain=ffn_gain, ffn_gate=ffn_gate, ffn_up=ffn_up, ffn_gate_scale=ffn_gate_scale, ffn_up_scale=ffn_up_scale, ffn_down=ffn_down, ffn_down_scale=ffn_down_scale)


EPS = 1e-06
RATE = 8.0

def rms_rows(rows, gain):
    values = rows.astype(jnp.float32)
    scale = lax.rsqrt(lax.optimization_barrier(jnp.mean(values * values, axis=-1, keepdims=True)) + EPS)
    return (values * scale * gain).astype(jnp.bfloat16)

def block_sum(acts, weight, blocks):
    width = acts.shape[1] // blocks
    total = jnp.zeros((acts.shape[0], weight.shape[1]), jnp.float32)
    for block in range(blocks):
        part = jnp.dot(acts[:, block * width:(block + 1) * width], weight[block * width:(block + 1) * width].astype(jnp.bfloat16), preferred_element_type=jnp.float32).astype(jnp.bfloat16)
        part = lax.optimization_barrier(part)
        total = total + part.astype(jnp.float32)
    return total

def combine(left, right):
    return (left[0] * right[0], right[0] * left[1] + right[1])

def recurrence(branch_in, branch_gate, conv_weight, recur_gate, input_gate, decay_rate, extra):
    length = branch_in.shape[0]
    taps = conv_weight.shape[0]
    values = branch_in.astype(jnp.float32)
    padded = jnp.pad(values, ((taps - 1, 0), (0, 0)))
    conv = jnp.zeros_like(values)
    for tap in range(taps):
        conv = conv + conv_weight[tap] * padded[tap:tap + length]
    nblocks, bdim = (recur_gate.shape[0], recur_gate.shape[1])
    grouped = conv.reshape(length, nblocks, bdim)
    recur = jax.nn.sigmoid(jnp.einsum('sni,nij->snj', grouped, recur_gate, precision=lax.Precision.HIGHEST).reshape(length, -1))
    ingate = jax.nn.sigmoid(jnp.einsum('sni,nij->snj', grouped, input_gate, precision=lax.Precision.HIGHEST).reshape(length, -1))
    log_rate = -RATE * jax.nn.softplus(-decay_rate) * recur - extra[:, None]
    factor = jnp.exp(log_rate)
    drive = jnp.sqrt(-jnp.expm1(2.0 * log_rate)) * (ingate * conv)
    state = lax.associative_scan(combine, (factor, drive), axis=0)[1]
    gelu_gate = jax.nn.gelu(branch_gate.astype(jnp.float32), approximate=True)
    return (state * gelu_gate).astype(jnp.bfloat16)

def reference(tokens, mix_gain, lru_input, lru_gate, lru_input_scale, lru_gate_scale, conv_weight, recur_gate, input_gate, decay_rate, extra_decay, lru_output, lru_output_scale, ffn_gain, ffn_gate, ffn_up, ffn_gate_scale, ffn_up_scale, ffn_down, ffn_down_scale):
    normed = rms_rows(tokens, mix_gain)
    branch_in = (jnp.dot(normed, lru_input.astype(jnp.bfloat16), preferred_element_type=jnp.float32) * lru_input_scale).astype(jnp.bfloat16)
    branch_gate = (jnp.dot(normed, lru_gate.astype(jnp.bfloat16), preferred_element_type=jnp.float32) * lru_gate_scale).astype(jnp.bfloat16)
    width = branch_in.shape[1]
    gated = jax.vmap(recurrence, in_axes=(0, 0, None, None, None, None, 0))(branch_in.reshape(SEQS, TOK_DEV, width), branch_gate.reshape(SEQS, TOK_DEV, width), conv_weight, recur_gate, input_gate, decay_rate, extra_decay.reshape(SEQS, TOK_DEV))
    gated = gated.reshape(TOKENS, width)
    mixed = (tokens.astype(jnp.float32) + block_sum(gated, lru_output, N_TP) * lru_output_scale).astype(jnp.bfloat16)
    normed2 = rms_rows(mixed, ffn_gain)
    gate_pre = jnp.dot(normed2, ffn_gate.astype(jnp.bfloat16), preferred_element_type=jnp.float32) * ffn_gate_scale
    up_pre = jnp.dot(normed2, ffn_up.astype(jnp.bfloat16), preferred_element_type=jnp.float32) * ffn_up_scale
    hidden = (jax.nn.silu(gate_pre) * up_pre).astype(jnp.bfloat16)
    total = block_sum(hidden, ffn_down, N_TP)
    return (mixed.astype(jnp.float32) + total * ffn_down_scale).astype(jnp.bfloat16)
```

```python
import functools

import jax
import jax.numpy as jnp
from jax import lax
from jax.experimental import pallas as pl
from jax.experimental.pallas import tpu as pltpu
from jax.sharding import PartitionSpec as P

EPS = 1e-06
RATE = 8.0
LANES = 128
MESH = pl.DeviceIdType.MESH
GROUPS = (4, 4, 3)
f32, bf16 = jnp.float32, jnp.bfloat16


def sigmoid(v):
    return 1.0 / (1.0 + jnp.exp(-v))


def layer_kernel(
    chunks, tok, piece, mix_gain, in_scale, gt_scale, conv_ref, map_ref, rate_ref, extra_ref,
    out_scale, ffn_gain, fg_scale, fu_scale, dn_scale, out_ref,
    W, X, N, BI, ST, GA, SB, RB, RB2, H, PS,
    send_sem, recv_sem, tp_send, tp_recv, own_sem,
):
    rep, fs, tp = lax.axis_index("rep"), lax.axis_index("fs"), lax.axis_index("tp")
    zl, y, x = fs // 16, (fs // 4) % 4, fs % 4
    rows, half = tok.shape
    up = lambda v: lax.rem(v + 1, 4)
    dn = lambda v: lax.rem(v + 3, 4)
    xl, xr, yl, yr = dn(x), up(x), dn(y), up(y)
    other = 1 - tp
    to_x = lambda v: (rep, zl * 16 + y * 4 + v, tp)
    to_y = lambda v: (rep, zl * 16 + v * 4 + x, tp)
    z_other = (1 - zl) * 16 + y * 4 + x
    z_next = (jnp.where(zl == 0, rep, 1 - rep), z_other, tp)
    z_prev = (jnp.where(zl == 0, 1 - rep, rep), z_other, tp)
    partner = (rep, fs, other)

    barrier = pltpu.get_barrier_semaphore()
    for peer in (to_x(xl), to_x(xr), to_y(yl), to_y(yr), z_next, z_prev, partner):
        pl.semaphore_signal(barrier, inc=1, device_id=peer, device_id_type=MESH)

    own = []
    for k, (start, width) in enumerate(chunks):
        cols = pl.ds(start, width)
        c = pltpu.make_async_copy(piece.at[:, cols], W.at[zl, y, x, :, cols], own_sem.at[k])
        c.start()
        own.append(c)
    keep = pltpu.make_async_copy(tok, X.at[tp], own_sem.at[len(chunks)])
    keep.start()

    def remote(src, dst, target, ssem, rsem):
        return pltpu.make_async_remote_copy(
            src_ref=src, dst_ref=dst, send_sem=ssem, recv_sem=rsem,
            device_id=target, device_id_type=MESH,
        )

    A, B = pl.ds(0, 32), pl.ds(32, 32)
    every = slice(None)

    def plan(k):
        cols = pl.ds(*chunks[k])
        at = lambda a, b, c, r: W.at[a, b, c, r, cols]
        return [
            [(at(zl, y, x, A), z_next), (at(zl, y, x, B), z_prev)],
            [
                (at(every, y, x, A), to_x(xr)), (at(every, y, x, A), to_x(xl)),
                (at(every, y, x, B), to_y(yr)), (at(every, y, x, B), to_y(yl)),
            ],
            [
                (at(0, y, xl, A), to_x(xr)), (at(1, y, xr, A), to_x(xl)),
                (at(0, yl, x, B), to_y(yr)), (at(1, yr, x, B), to_y(yl)),
            ],
            [
                (at(every, y, every, A), to_y(yr)), (at(every, y, every, A), to_y(yl)),
                (at(every, every, x, B), to_x(xr)), (at(every, every, x, B), to_x(xl)),
            ],
            [
                (at(0, yl, every, A), to_y(yr)), (at(1, yr, every, A), to_y(yl)),
                (at(0, every, xl, B), to_x(xr)), (at(1, every, xr, B), to_x(xl)),
            ],
        ]

    flights = {}

    def issue(k, s):
        if k >= len(chunks):
            return
        if s == 0:
            own[k].wait()
        else:
            land(k, s - 1)
        base = sum(len(p) for p in plan(k)[:s])
        flights[k, s] = []
        for i, (ref, target) in enumerate(plan(k)[s]):
            c = remote(ref, ref, target, send_sem.at[k, base + i], recv_sem.at[k, base + i])
            c.start()
            flights[k, s].append(c)

    def land(k, s):
        for c in flights[k, s]:
            c.wait_recv()

    pl.semaphore_wait(barrier, 7)
    swap_tok = remote(tok, X.at[tp], partner, tp_send.at[0], tp_recv.at[0])
    swap_tok.start()
    for k in range(len(chunks)):
        issue(k, 0)
    issue(0, 1)
    issue(1, 1)
    keep.wait()
    swap_tok.wait_recv()

    def norm_rows(gain):
        step = 64

        def body(i, carry):
            r = pl.ds(pl.multiple_of(i * step, step), step)
            lo, hi = X[0, r, :].astype(f32), X[1, r, :].astype(f32)
            total = jnp.sum(lo * lo, axis=-1, keepdims=True) + jnp.sum(
                hi * hi, axis=-1, keepdims=True
            )
            scale = lax.rsqrt(total / (2 * half) + EPS)
            N[r, :half] = (lo * scale * gain[:, :half]).astype(bf16)
            N[r, half:] = (hi * scale * gain[:, half:]).astype(bf16)
            return carry

        lax.fori_loop(0, rows // step, body, 0)

    def wide(start, width):
        return W[:, :, :, :, pl.ds(start, width)].reshape(2 * half, width)

    def dot(a, b):
        return jnp.dot(a, b, preferred_element_type=f32)

    def dot_t(a, b):
        return lax.dot_general(a, b, (((1,), (1,)), ((), ())), preferred_element_type=f32)

    def branch_in():
        def body(i, carry):
            c = pl.multiple_of(i * 256, 256)
            BI[:, pl.ds(c, 256)] = (
                dot(N[...], wide(c, 256)) * in_scale[:, pl.ds(c, 256)]
            ).astype(bf16)
            return carry

        lax.fori_loop(0, half // 256, body, 0)

    def scan_block(i, carry):
        cols = pl.ds(pl.multiple_of(i * LANES, LANES), LANES)
        length = rows
        taps = conv_ref.shape[0]
        values = BI[:, cols].astype(f32)
        weights = conv_ref[:, cols]
        row = lax.broadcasted_iota(jnp.int32, values.shape, 0)
        conv = weights[taps - 1 : taps, :] * values
        for back in range(1, taps):
            moved = jnp.where(row >= back, pltpu.roll(values, back, 0), 0.0)
            conv = conv + weights[taps - 1 - back : taps - back, :] * moved
        mapped = jnp.dot(
            conv, map_ref[i], preferred_element_type=f32, precision=lax.Precision.HIGHEST
        )
        recur = sigmoid(mapped[:, :LANES])
        ingate = sigmoid(mapped[:, LANES:])
        log_rate = rate_ref[:, cols] * recur - extra_ref[...]
        a = jnp.exp(log_rate)
        u = -2.0 * log_rate
        series = u * (1 - u / 2 * (1 - u / 3 * (1 - u / 4 * (1 - u / 5 * (1 - u / 6)))))
        b = jnp.sqrt(jnp.where(u < 0.25, series, 1.0 - jnp.exp(-u))) * (ingate * conv)
        inner = row % 8
        for s in (1, 2, 4):
            live = inner >= s
            b = jnp.where(live, a * pltpu.roll(b, s, 0) + b, b)
            a = jnp.where(live, a * pltpu.roll(a, s, 0), a)
        groups = length // 8
        last_a = a.reshape(groups, 8, LANES)
        last_b = b.reshape(groups, 8, LANES)
        ca = jnp.broadcast_to(last_a[:, 7:8, :], last_a.shape).reshape(length, LANES)
        cb = jnp.broadcast_to(last_b[:, 7:8, :], last_b.shape).reshape(length, LANES)
        s = 8
        while s < length:
            cb_new = ca[s:] * cb[:-s] + cb[s:]
            ca_new = ca[s:] * ca[:-s]
            cb = jnp.concatenate([cb[:s], cb_new], axis=0)
            ca = jnp.concatenate([ca[:s], ca_new], axis=0)
            s *= 2
        ST[:, cols] = jnp.concatenate([b[:8], a[8:] * cb[:-8] + b[8:]], axis=0)
        return carry

    def gate_block(i, carry):
        c = pl.multiple_of(i * 256, 256)
        cols = pl.ds(c, 256)
        acc = dot(N[...], wide(pl.multiple_of(half + c, 256), 256)) * gt_scale[:, cols]
        g = acc.astype(bf16).astype(f32)
        gelu = 0.5 * g * (1.0 + jnp.tanh(0.7978845608028654 * (g + 0.044715 * g * g * g)))
        GA[:, cols] = (ST[:, cols] * gelu).astype(bf16)
        return carry

    def rows_of(block, j, start, width):
        return W[block, j, :, :, pl.ds(start, width)].reshape(256, width)

    def mixer_out():
        def send_body(j, carry):
            cols = pl.ds(pl.multiple_of(j * 256, 256), 256)
            SB[:, cols] = dot_t(GA[...], rows_of(other, j, 2 * half, half)).astype(bf16)
            return carry

        def mine_body(j, carry):
            cols = pl.ds(pl.multiple_of(j * 256, 256), 256)
            PS[0, :, cols] = dot_t(GA[...], rows_of(tp, j, 2 * half, half))
            return carry

        lax.fori_loop(0, 4, send_body, 0)
        swap = remote(SB, RB, partner, tp_send.at[1], tp_recv.at[1])
        swap.start()
        lax.fori_loop(0, 4, mine_body, 0)
        swap.wait_recv()

        def mixed_body(i, carry):
            r = pl.ds(pl.multiple_of(i * 64, 64), 64)
            total = PS[0, r, :] + RB[r, :].astype(f32)
            X[tp, r, :] = (tok[r, :].astype(f32) + total * out_scale[...]).astype(bf16)
            return carry

        lax.fori_loop(0, rows // 64, mixed_body, 0)
        swap.wait_send()
        share = remote(X.at[tp], X.at[tp], partner, tp_send.at[2], tp_recv.at[2])
        share.start()
        share.wait()
        norm_rows(ffn_gain)

    def hidden_tile(unit, start):
        cols = pl.ds(pl.multiple_of(unit * LANES, LANES), LANES)
        both = dot(N[...], wide(start, 256))
        gate = both[:, :LANES] * fg_scale[:, cols]
        lift = both[:, LANES:] * fu_scale[:, cols]
        H[:, cols] = (gate / (1.0 + jnp.exp(-gate)) * lift).astype(bf16)

    def ffn(g):
        first, count = sum(GROUPS[:g]), GROUPS[g]
        start = 3 * half + first * 3 * LANES
        lax.fori_loop(
            0, count,
            lambda t, c: (hidden_tile(first + t, pl.multiple_of(start + t * 256, 128)), c)[1], 0,
        )
        down = start + count * 256
        acts = lambda: H[:, first * LANES : (first + count) * LANES]

        def part(slot, block, j):
            cols = pl.ds(pl.multiple_of(j * 256, 256), 256)
            v = dot_t(acts(), rows_of(block, j, down, count * LANES))
            if g > 0:
                v = PS[slot, :, cols] + v
            return cols, v

        last = g == len(GROUPS) - 1

        def away(j, carry):
            cols, v = part(1, other, j)
            if last:
                SB[:, cols] = v.astype(bf16)
            else:
                PS[1, :, cols] = v
            return carry

        def home(j, carry):
            cols, v = part(0, tp, j)
            PS[0, :, cols] = v
            return carry

        lax.fori_loop(0, 4, away, 0)
        if last:
            swap = remote(SB, RB2, partner, tp_send.at[3], tp_recv.at[3])
            swap.start()
        lax.fori_loop(0, 4, home, 0)
        if last:
            swap.wait()

            def final(i, carry):
                r = pl.ds(pl.multiple_of(i * 64, 64), 64)
                total = PS[0, r, :] + RB2[r, :].astype(f32)
                out_ref[r, :] = (X[tp, r, :].astype(f32) + total * dn_scale[...]).astype(bf16)
                return carry

            lax.fori_loop(0, rows // 64, final, 0)

    issue(0, 2)
    norm_rows(mix_gain)
    issue(1, 2)
    issue(0, 3)
    issue(2, 1)
    issue(0, 4)
    issue(1, 3)
    issue(2, 2)
    issue(3, 1)
    land(0, 4)
    branch_in()
    lax.fori_loop(0, 2, scan_block, 0)
    issue(1, 4)
    issue(2, 3)
    issue(3, 2)
    issue(4, 1)
    lax.fori_loop(2, 5, scan_block, 0)
    land(1, 4)
    issue(2, 4)
    issue(3, 3)
    issue(4, 2)
    issue(5, 1)
    lax.fori_loop(5, 8, scan_block, 0)
    lax.fori_loop(0, 4, gate_block, 0)
    issue(3, 4)
    issue(4, 3)
    issue(5, 2)
    land(2, 4)
    mixer_out()
    issue(4, 4)
    issue(5, 3)
    land(3, 4)
    ffn(0)
    issue(5, 4)
    land(4, 4)
    ffn(1)
    land(5, 4)
    ffn(2)
    swap_tok.wait_send()
    for group in flights.values():
        for c in group:
            c.wait_send()


def local(*args):
    (
        tokens, mix_gain, lru_input, lru_gate, lru_input_scale, lru_gate_scale, conv_weight,
        recur_gate, input_gate, decay_rate, extra_decay, lru_output, lru_output_scale, ffn_gain,
        ffn_gate, ffn_up, ffn_gate_scale, ffn_up_scale, ffn_down, ffn_down_scale,
    ) = args
    tp = lax.axis_index("tp")
    rows, half = tokens.shape
    units = ffn_gate.shape[1] // LANES

    out_t = lru_output.astype(bf16).T
    down_t = ffn_down.astype(bf16).T
    gate16, up16 = ffn_gate.astype(bf16), ffn_up.astype(bf16)
    parts = [lru_input.astype(bf16), lru_gate.astype(bf16), out_t]
    chunks = [(0, half), (half, half), (2 * half, half)]
    first = 0
    for count in GROUPS:
        for t in range(first, first + count):
            cut = slice(t * LANES, (t + 1) * LANES)
            parts += [gate16[:, cut], up16[:, cut]]
        parts.append(down_t[:, first * LANES : (first + count) * LANES])
        chunks.append((3 * half + first * 3 * LANES, count * 3 * LANES))
        first += count
    assert first == units
    piece = jnp.concatenate(parts, axis=1)
    width = piece.shape[1]

    per = LANES // recur_gate.shape[1]
    groups = recur_gate.shape[0] // per

    def block_diag(blocks):
        tall = blocks.reshape(groups, LANES, blocks.shape[2])
        both = jnp.concatenate([tall] * per, axis=2)
        r = lax.broadcasted_iota(jnp.int32, both.shape, 1) // blocks.shape[1]
        c = lax.broadcasted_iota(jnp.int32, both.shape, 2) // blocks.shape[2]
        return jnp.where(r == c, both, 0.0)

    maps = jnp.concatenate([block_diag(recur_gate), block_diag(input_gate)], axis=2)
    rate = (-RATE * jax.nn.softplus(-decay_rate))[None, :]
    mine = lambda v: lax.dynamic_slice_in_dim(v, tp * half, half)[None, :]
    n = len(chunks)
    vmem = pl.BlockSpec(memory_space=pltpu.VMEM)
    return pl.pallas_call(
        functools.partial(layer_kernel, tuple(chunks)),
        out_shape=jax.ShapeDtypeStruct((rows, half), bf16),
        in_specs=[vmem, pl.BlockSpec(memory_space=pl.ANY)] + [vmem] * 12,
        out_specs=vmem,
        scratch_shapes=[
            pltpu.VMEM((2, 4, 4, 64, width), bf16),
            pltpu.VMEM((2, rows, half), bf16),
            pltpu.VMEM((rows, 2 * half), bf16),
            pltpu.VMEM((rows, half), bf16),
            pltpu.VMEM((rows, half), f32),
            pltpu.VMEM((rows, half), bf16),
            pltpu.VMEM((rows, half), bf16),
            pltpu.VMEM((rows, half), bf16),
            pltpu.VMEM((rows, half), bf16),
            pltpu.VMEM((rows, units * LANES), bf16),
            pltpu.VMEM((2, rows, half), f32),
            pltpu.SemaphoreType.DMA((n, 18)),
            pltpu.SemaphoreType.DMA((n, 18)),
            pltpu.SemaphoreType.DMA((4,)),
            pltpu.SemaphoreType.DMA((4,)),
            pltpu.SemaphoreType.DMA((n + 1,)),
        ],
        compiler_params=pltpu.CompilerParams(
            collective_id=0, has_side_effects=True, vmem_limit_bytes=67043328
        ),
        name="layer",
    )(
        tokens, piece, mix_gain[None, :], lru_input_scale[None, :], lru_gate_scale[None, :],
        conv_weight, maps, rate, extra_decay[:, None], mine(lru_output_scale), ffn_gain[None, :],
        ffn_gate_scale[None, :], ffn_up_scale[None, :], mine(ffn_down_scale),
    )


def solution(mesh):
    in_specs = (
        P(("rep", "fs"), "tp"), P(), P("fs", "tp"), P("fs", "tp"), P("tp"), P("tp"),
        P(None, "tp"), P("tp", None, None), P("tp", None, None), P("tp"), P(("rep", "fs")),
        P("tp", "fs"), P(), P(), P("fs", "tp"), P("fs", "tp"), P("tp"), P("tp"), P("tp", "fs"),
        P(),
    )
    return jax.shard_map(
        local, mesh=mesh, in_specs=in_specs, out_specs=P(("rep", "fs"), "tp"), check_vma=False
    )
```

```python
import functools

import jax
import jax.numpy as jnp
from jax import lax
from jax.experimental import pallas as pl
from jax.experimental.pallas import tpu as pltpu
from jax.sharding import PartitionSpec as P

EPS = 1e-06
RATE = 8.0
LANES = 128
MESH = pl.DeviceIdType.MESH
GROUPS = (4, 4, 3)
f32, bf16 = jnp.float32, jnp.bfloat16


def sigmoid(v):
    return 1.0 / (1.0 + jnp.exp(-v))


def layer_kernel(
    chunks, tok, w_in, w_gate, w_out, w_fg, w_fu, w_dn,
    mix_gain, in_scale, gt_scale, conv_ref, recur_ref, ingate_ref, decay_ref, extra_ref,
    out_scale, ffn_gain, fg_scale, fu_scale, dn_scale, out_ref,
    W, X, N, BI, ST, GA, SB, RB, RB2, H, PS, F1, F2, F3, F4, F5, F6, MAP, RATES, EX,
    send_sem, recv_sem, tp_send, tp_recv, own_sem,
):
    rep, fs, tp = lax.axis_index("rep"), lax.axis_index("fs"), lax.axis_index("tp")
    zl, y, x = fs // 16, (fs // 4) % 4, fs % 4
    rows, half = tok.shape
    n = len(chunks)
    up = lambda v: lax.rem(v + 1, 4)
    dn = lambda v: lax.rem(v + 3, 4)
    xl, xr, yl, yr = dn(x), up(x), dn(y), up(y)
    other, away_zl = 1 - tp, 1 - zl
    to_x = lambda v: (rep, zl * 16 + y * 4 + v, tp)
    to_y = lambda v: (rep, zl * 16 + v * 4 + x, tp)
    z_other = away_zl * 16 + y * 4 + x
    rep_next = jnp.where(zl == 0, rep, 1 - rep)
    rep_prev = 1 - rep_next
    z_next, z_prev = (rep_next, z_other, tp), (rep_prev, z_other, tp)
    partner = (rep, fs, other)

    barrier = pltpu.get_barrier_semaphore()
    for peer in (to_x(xl), to_x(xr), to_y(yl), to_y(yr), z_next, z_prev, partner):
        pl.semaphore_signal(barrier, inc=1, device_id=peer, device_id_type=MESH)

    loads = []
    for i, (src, dst) in enumerate(
        [(w_in, F1), (w_gate, F2), (w_out, F3), (w_fg, F4), (w_fu, F5), (w_dn, F6)]
    ):
        c = pltpu.make_async_copy(src, dst, own_sem.at[i])
        c.start()
        loads.append(c)
    keep = pltpu.make_async_copy(tok, X.at[tp], own_sem.at[6])
    keep.start()

    def remote(src, dst, target, ssem, rsem):
        return pltpu.make_async_remote_copy(
            src_ref=src, dst_ref=dst, send_sem=ssem, recv_sem=rsem,
            device_id=target, device_id_type=MESH,
        )

    A, B = pl.ds(0, 32), pl.ds(32, 32)
    every = slice(None)
    lo2, hi2 = pl.ds(0, 2), pl.ds(2, 2)
    mine_rows = pl.ds(pl.multiple_of(rep * 32, 32), 32)
    CA = pl.ds(pl.multiple_of(rep * 32, 16), 16)
    CB = pl.ds(pl.multiple_of(rep * 32 + 16, 16), 16)
    next_rows = pl.ds(pl.multiple_of(rep_next * 32, 32), 32)
    prev_rows = pl.ds(pl.multiple_of(rep_prev * 32, 32), 32)
    up_x, dn_x, up_y, dn_y = to_x(xr), to_x(xl), to_y(yr), to_y(yl)
    needs = {
        "z0": (), "s1": ("z0",), "s2": ("s1",), "s3a": ("s2",), "s3b": ("s2",), "s4": ("s3a",),
        "c1": (), "c2": ("c1",), "c3": ("c2",), "c4": ("c3",), "c5a": ("c4",), "c5b": ("c4",),
        "c6": ("c5a",),
    }

    def plan(k):
        start, width, last = chunks[k]
        cols, tail = pl.ds(start, width - last), pl.ds(start + width - last, last)
        cut = (last // LANES + 1) // 2 * LANES
        t1 = pl.ds(start + width - last, cut)
        t2 = pl.ds(start + width - last + cut, last - cut)
        at = lambda a, b, c, r: W.at[a, b, c, r, cols]
        ct = lambda a, b, c, r, t=tail: W.at[a, b, c, r, t]
        return {
            "z0": [(at(zl, y, x, A), z_next), (at(zl, y, x, B), z_prev)],
            "s1": [
                (at(every, y, x, A), up_x), (at(every, y, x, A), dn_x),
                (at(every, y, x, B), up_y), (at(every, y, x, B), dn_y),
            ],
            "s2": [
                (at(0, y, xl, A), up_x), (at(1, y, xr, A), dn_x),
                (at(0, yl, x, B), up_y), (at(1, yr, x, B), dn_y),
            ],
            "s3a": [
                (at(0, y, every, A), up_y), (at(1, y, every, A), dn_y),
                (at(0, every, x, B), up_x), (at(1, every, x, B), dn_x),
            ],
            "s3b": [
                (at(1, y, every, A), up_y), (at(0, y, every, A), dn_y),
                (at(1, every, x, B), up_x), (at(0, every, x, B), dn_x),
            ],
            "s4": [
                (at(0, yl, every, A), up_y), (at(1, yr, every, A), dn_y),
                (at(0, every, xl, B), up_x), (at(1, every, xr, B), dn_x),
            ],
            "c1": [
                (ct(zl, y, x, CA), up_x), (ct(zl, y, x, CA), dn_x),
                (ct(zl, y, x, CB), up_y), (ct(zl, y, x, CB), dn_y),
            ],
            "c2": [
                (ct(zl, y, xl, CA, t1), up_x), (ct(zl, y, xr, CA, t2), dn_x),
                (ct(zl, yl, x, CB, t1), up_y), (ct(zl, yr, x, CB, t2), dn_y),
            ],
            "c3": [
                (ct(zl, y, every, CA), up_y), (ct(zl, y, every, CA), dn_y),
                (ct(zl, every, x, CB), up_x), (ct(zl, every, x, CB), dn_x),
            ],
            "c4": [
                (ct(zl, yl, lo2, CA), up_y), (ct(zl, yr, hi2, CA), dn_y),
                (ct(zl, lo2, xl, CB), up_x), (ct(zl, hi2, xr, CB), dn_x),
            ],
            "c5a": [
                (ct(zl, lo2, every, mine_rows), z_next), (ct(zl, hi2, every, mine_rows), z_prev),
            ],
            "c5b": [
                (ct(zl, hi2, every, mine_rows), z_next), (ct(zl, lo2, every, mine_rows), z_prev),
            ],
            "c6": [
                (ct(away_zl, lo2, every, prev_rows), z_next),
                (ct(away_zl, hi2, every, next_rows), z_prev),
            ],
        }

    flights, landed = {}, set()

    def land(k, s):
        if (k, s) not in landed:
            landed.add((k, s))
            for c in flights[k, s]:
                c.wait_recv()

    def go(k, *names):
        if k >= n:
            return
        steps = plan(k)
        order = list(steps)
        for s in names:
            for before in needs[s]:
                land(k, before)
            base = sum(len(steps[o]) for o in order[: order.index(s)])
            flights[k, s] = []
            for i, (ref, target) in enumerate(steps[s]):
                c = remote(ref, ref, target, send_sem.at[k, base + i], recv_sem.at[k, base + i])
                c.start()
                flights[k, s].append(c)

    def done(k):
        for s in needs:
            land(k, s)

    def stage_weights(k):
        start = chunks[k][0]

        def put(at, value):
            W[zl, y, x, :, pl.ds(at, value.shape[1])] = value.astype(bf16)

        if k < 2:
            loads[k].wait()
            put(start, (F1, F2)[k][...])
        elif k == 2:
            loads[2].wait()
            put(start, F3[...].T)
        else:
            if k == 3:
                for c in loads[3:]:
                    c.wait()
            first, count = sum(GROUPS[: k - 3]), GROUPS[k - 3]
            for t in range(count):
                cut = slice((first + t) * LANES, (first + t + 1) * LANES)
                put(start + t * 256, F4[:, cut])
                put(start + t * 256 + LANES, F5[:, cut])
            put(start + count * 256, F6[first * LANES : (first + count) * LANES, :].T)

    stage_weights(0)
    pl.semaphore_wait(barrier, 7)
    swap_tok = remote(tok, X.at[tp], partner, tp_send.at[0], tp_recv.at[0])
    swap_tok.start()
    go(0, "c1", "z0")
    stage_weights(1)
    stage_weights(2)
    go(1, "c1", "z0")
    go(0, "s1", "c2")
    stage_weights(3)
    go(2, "z0")
    go(0, "s2", "c3")
    stage_weights(4)
    go(3, "z0")
    stage_weights(5)
    go(4, "z0")
    go(0, "s3a", "s3b", "c4")
    go(5, "z0")

    def prepare():
        zeros = jnp.zeros((64, 64), f32)
        for g in range(half // LANES):
            for p in range(2):
                r = recur_ref[2 * g + p]
                q = ingate_ref[2 * g + p]
                parts = [r, zeros, q, zeros] if p == 0 else [zeros, r, zeros, q]
                MAP[g, p * 64 : p * 64 + 64, :] = jnp.concatenate(parts, axis=1)
        v = -decay_ref[...]
        RATES[...] = -RATE * (jnp.maximum(v, 0.0) + jnp.log1p(jnp.exp(-jnp.abs(v))))
        EX[...] = jnp.broadcast_to(extra_ref[...], (LANES, rows)).T

    prepare()
    keep.wait()
    swap_tok.wait_recv()

    def norm_rows(gain):
        step = 64

        def body(i, carry):
            r = pl.ds(pl.multiple_of(i * step, step), step)
            lo, hi = X[0, r, :].astype(f32), X[1, r, :].astype(f32)
            total = jnp.sum(lo * lo, axis=-1, keepdims=True) + jnp.sum(
                hi * hi, axis=-1, keepdims=True
            )
            scale = lax.rsqrt(total / (2 * half) + EPS)
            N[r, :half] = (lo * scale * gain[:, :half]).astype(bf16)
            N[r, half:] = (hi * scale * gain[:, half:]).astype(bf16)
            return carry

        lax.fori_loop(0, rows // step, body, 0)

    def wide(start, width):
        return W[:, :, :, :, pl.ds(start, width)].reshape(2 * half, width)

    def dot(a, b):
        return jnp.dot(a, b, preferred_element_type=f32)

    def dot_t(a, b):
        return lax.dot_general(a, b, (((1,), (1,)), ((), ())), preferred_element_type=f32)

    def branch_in():
        def body(i, carry):
            c = pl.multiple_of(i * 256, 256)
            BI[:, pl.ds(c, 256)] = (
                dot(N[...], wide(c, 256)) * in_scale[:, pl.ds(c, 256)]
            ).astype(bf16)
            return carry

        lax.fori_loop(0, half // 256, body, 0)

    def scan_block(i, carry):
        cols = pl.ds(pl.multiple_of(i * LANES, LANES), LANES)
        length = rows
        taps = conv_ref.shape[0]
        values = BI[:, cols].astype(f32)
        weights = conv_ref[:, cols]
        row = lax.broadcasted_iota(jnp.int32, values.shape, 0)
        conv = weights[taps - 1 : taps, :] * values
        for back in range(1, taps):
            moved = jnp.where(row >= back, pltpu.roll(values, back, 0), 0.0)
            conv = conv + weights[taps - 1 - back : taps - back, :] * moved
        mapped = jnp.dot(
            conv, MAP[i], preferred_element_type=f32, precision=lax.Precision.HIGHEST
        )
        recur = sigmoid(mapped[:, :LANES])
        ingate = sigmoid(mapped[:, LANES:])
        log_rate = RATES[:, cols] * recur - EX[...]
        a = jnp.exp(log_rate)
        u = -2.0 * log_rate
        series = u * (1 - u / 2 * (1 - u / 3 * (1 - u / 4 * (1 - u / 5 * (1 - u / 6)))))
        b = jnp.sqrt(jnp.where(u < 0.25, series, 1.0 - jnp.exp(-u))) * (ingate * conv)
        inner = row % 8
        for s in (1, 2, 4):
            live = inner >= s
            b = jnp.where(live, a * pltpu.roll(b, s, 0) + b, b)
            a = jnp.where(live, a * pltpu.roll(a, s, 0), a)
        groups = length // 8
        last_a = a.reshape(groups, 8, LANES)
        last_b = b.reshape(groups, 8, LANES)
        ca = jnp.broadcast_to(last_a[:, 7:8, :], last_a.shape).reshape(length, LANES)
        cb = jnp.broadcast_to(last_b[:, 7:8, :], last_b.shape).reshape(length, LANES)
        s = 8
        while s < length:
            cb_new = ca[s:] * cb[:-s] + cb[s:]
            ca_new = ca[s:] * ca[:-s]
            cb = jnp.concatenate([cb[:s], cb_new], axis=0)
            ca = jnp.concatenate([ca[:s], ca_new], axis=0)
            s *= 2
        ST[:, cols] = jnp.concatenate([b[:8], a[8:] * cb[:-8] + b[8:]], axis=0)
        return carry

    def gate_block(i, carry):
        c = pl.multiple_of(i * 256, 256)
        cols = pl.ds(c, 256)
        acc = dot(N[...], wide(pl.multiple_of(half + c, 256), 256)) * gt_scale[:, cols]
        g = acc.astype(bf16).astype(f32)
        gelu = 0.5 * g * (1.0 + jnp.tanh(0.7978845608028654 * (g + 0.044715 * g * g * g)))
        GA[:, cols] = (ST[:, cols] * gelu).astype(bf16)
        return carry

    def rows_of(block, j, start, width):
        return W[block, j, :, :, pl.ds(start, width)].reshape(256, width)

    def mixer_out():
        def send_body(j, carry):
            cols = pl.ds(pl.multiple_of(j * 256, 256), 256)
            SB[:, cols] = dot_t(GA[...], rows_of(other, j, 2 * half, half)).astype(bf16)
            return carry

        def mine_body(j, carry):
            cols = pl.ds(pl.multiple_of(j * 256, 256), 256)
            PS[0, :, cols] = dot_t(GA[...], rows_of(tp, j, 2 * half, half))
            return carry

        lax.fori_loop(0, 4, send_body, 0)
        swap = remote(SB, RB, partner, tp_send.at[1], tp_recv.at[1])
        swap.start()
        lax.fori_loop(0, 4, mine_body, 0)
        return swap

    own_cols = pl.ds(pl.multiple_of(tp * half, half), half)

    def mixer_mixed(swap):
        swap.wait_recv()

        def mixed_body(i, carry):
            r = pl.ds(pl.multiple_of(i * 64, 64), 64)
            total = PS[0, r, :] + RB[r, :].astype(f32)
            X[tp, r, :] = (tok[r, :].astype(f32) + total * out_scale[:, own_cols]).astype(bf16)
            return carry

        lax.fori_loop(0, rows // 64, mixed_body, 0)
        swap.wait_send()
        share = remote(X.at[tp], X.at[tp], partner, tp_send.at[2], tp_recv.at[2])
        share.start()
        return share

    def hidden_tile(unit, start):
        cols = pl.ds(pl.multiple_of(unit * LANES, LANES), LANES)
        both = dot(N[...], wide(start, 256))
        gate = both[:, :LANES] * fg_scale[cols].reshape(1, LANES)
        lift = both[:, LANES:] * fu_scale[cols].reshape(1, LANES)
        H[:, cols] = (gate / (1.0 + jnp.exp(-gate)) * lift).astype(bf16)

    def ffn(g):
        first, count = sum(GROUPS[:g]), GROUPS[g]
        start = 3 * half + first * 3 * LANES
        lax.fori_loop(
            0, count,
            lambda t, c: (hidden_tile(first + t, pl.multiple_of(start + t * 256, 128)), c)[1], 0,
        )
        down = start + count * 256
        acts = lambda: H[:, first * LANES : (first + count) * LANES]

        def part(slot, block, j):
            cols = pl.ds(pl.multiple_of(j * 256, 256), 256)
            v = dot_t(acts(), rows_of(block, j, down, count * LANES))
            if g > 0:
                v = PS[slot, :, cols] + v
            return cols, v

        last = g == len(GROUPS) - 1

        def away(j, carry):
            cols, v = part(1, other, j)
            if last:
                SB[:, cols] = v.astype(bf16)
            else:
                PS[1, :, cols] = v
            return carry

        def home(j, carry):
            cols, v = part(0, tp, j)
            PS[0, :, cols] = v
            return carry

        lax.fori_loop(0, 4, away, 0)
        if last:
            swap = remote(SB, RB2, partner, tp_send.at[3], tp_recv.at[3])
            swap.start()
        lax.fori_loop(0, 4, home, 0)
        if last:
            swap.wait()

            def final(i, carry):
                r = pl.ds(pl.multiple_of(i * 64, 64), 64)
                total = PS[0, r, :] + RB2[r, :].astype(f32)
                out_ref[r, :] = (X[tp, r, :].astype(f32) + total * dn_scale[:, own_cols]).astype(bf16)
                return carry

            lax.fori_loop(0, rows // 64, final, 0)

    def slot_a(k):
        go(k + 1, "c4")
        go(k + 2, "c2")
        go(k, "s3a", "s3b")
        go(k + 1, "s2")
        go(k + 2, "s1")
        go(k, "c6")

    def slot_b(k):
        go(k + 2, "c3")
        go(k + 3, "c1")
        go(k, "s4")
        go(k + 1, "c5a", "c5b")

    def scans(first, last):
        lax.fori_loop(first, last, scan_block, 0)

    go(0, "c5a", "c5b")
    go(1, "s1", "c2")
    go(2, "c1", "s1")
    norm_rows(mix_gain)
    go(0, "s4")
    go(1, "c3", "s2")
    go(2, "c2")
    go(0, "c6")
    go(1, "c4")
    go(2, "c3")
    go(3, "c1")
    go(1, "c5a", "c5b")
    go(2, "c4")
    go(3, "c2")
    go(1, "s3a", "s3b")
    go(2, "s2")
    go(3, "s1")
    done(0)
    branch_in()
    go(1, "c6")
    slot_b(1)
    scans(0, 3)
    slot_a(2)
    scans(3, 5)
    slot_b(2)
    scans(5, 8)
    done(1)
    lax.fori_loop(0, 4, gate_block, 0)
    slot_a(3)
    done(2)
    swap = mixer_out()
    slot_b(3)
    share = mixer_mixed(swap)
    slot_a(4)
    share.wait()
    norm_rows(ffn_gain)
    done(3)
    ffn(0)
    slot_b(4)
    slot_a(5)
    done(4)
    ffn(1)
    slot_b(5)
    done(5)
    ffn(2)
    swap_tok.wait_send()
    for group in flights.values():
        for c in group:
            c.wait_send()


def local(*args):
    (
        tokens, mix_gain, lru_input, lru_gate, lru_input_scale, lru_gate_scale, conv_weight,
        recur_gate, input_gate, decay_rate, extra_decay, lru_output, lru_output_scale, ffn_gain,
        ffn_gate, ffn_up, ffn_gate_scale, ffn_up_scale, ffn_down, ffn_down_scale,
    ) = args
    rows, half = tokens.shape
    units = ffn_gate.shape[1] // LANES
    chunks = [(k * half, half, 3 * LANES) for k in range(3)]
    first = 0
    for count in GROUPS:
        chunks.append((3 * half + first * 3 * LANES, count * 3 * LANES, (count + 1) * LANES))
        first += count
    assert first == units
    width = 3 * half + 3 * LANES * units
    n = len(chunks)
    row = lambda v: v[None, :]
    vmem = pl.BlockSpec(memory_space=pltpu.VMEM)
    hbm = pl.BlockSpec(memory_space=pl.ANY)
    return pl.pallas_call(
        functools.partial(layer_kernel, tuple(chunks)),
        out_shape=jax.ShapeDtypeStruct((rows, half), bf16),
        in_specs=[vmem] + [hbm] * 6 + [vmem] * 13,
        out_specs=vmem,
        scratch_shapes=[
            pltpu.VMEM((2, 4, 4, 64, width), bf16),
            pltpu.VMEM((2, rows, half), bf16),
            pltpu.VMEM((rows, 2 * half), bf16),
            pltpu.VMEM((rows, half), bf16),
            pltpu.VMEM((rows, half), f32),
            pltpu.VMEM((rows, half), bf16),
            pltpu.VMEM((rows, half), bf16),
            pltpu.VMEM((rows, half), bf16),
            pltpu.VMEM((rows, half), bf16),
            pltpu.VMEM((rows, units * LANES), bf16),
            pltpu.VMEM((2, rows, half), f32),
            pltpu.VMEM(lru_input.shape, f32),
            pltpu.VMEM(lru_gate.shape, f32),
            pltpu.VMEM(lru_output.shape, f32),
            pltpu.VMEM(ffn_gate.shape, f32),
            pltpu.VMEM(ffn_up.shape, f32),
            pltpu.VMEM(ffn_down.shape, f32),
            pltpu.VMEM((half // LANES, LANES, 2 * LANES), f32),
            pltpu.VMEM((1, half), f32),
            pltpu.VMEM((rows, LANES), f32),
            pltpu.SemaphoreType.DMA((n, 44)),
            pltpu.SemaphoreType.DMA((n, 44)),
            pltpu.SemaphoreType.DMA((4,)),
            pltpu.SemaphoreType.DMA((4,)),
            pltpu.SemaphoreType.DMA((7,)),
        ],
        compiler_params=pltpu.CompilerParams(
            collective_id=0, has_side_effects=True, vmem_limit_bytes=67043328
        ),
        name="layer",
    )(
        tokens, lru_input, lru_gate, lru_output, ffn_gate, ffn_up, ffn_down, row(mix_gain),
        row(lru_input_scale), row(lru_gate_scale), conv_weight, recur_gate, input_gate,
        row(decay_rate), row(extra_decay), row(lru_output_scale), row(ffn_gain),
        ffn_gate_scale, ffn_up_scale, row(ffn_down_scale),
    )


def solution(mesh):
    in_specs = (
        P(("rep", "fs"), "tp"), P(), P("fs", "tp"), P("fs", "tp"), P("tp"), P("tp"),
        P(None, "tp"), P("tp", None, None), P("tp", None, None), P("tp"), P(("rep", "fs")),
        P("tp", "fs"), P(), P(), P("fs", "tp"), P("fs", "tp"), P("tp"), P("tp"), P("tp", "fs"),
        P(),
    )
    return jax.shard_map(
        local, mesh=mesh, in_specs=in_specs, out_specs=P(("rep", "fs"), "tp"), check_vma=False
    )
```

```python
import functools

import jax
import jax.numpy as jnp
from jax import lax
from jax.experimental import pallas as pl
from jax.experimental.pallas import tpu as pltpu
from jax.sharding import PartitionSpec as P

EPS = 1e-06
RATE = 8.0
LANES = 128
MESH = pl.DeviceIdType.MESH
NEEDS = {
    "z0": (), "s1": ("z0",), "s2": ("s1",), "s3a": ("s2",), "s3b": ("s2",), "s4": ("s3a",),
    "c1": (), "c2": ("c1",), "c3": ("c2",), "c4": ("c3",), "c5a": ("c4",), "c5b": ("c4",),
    "c6": ("c5a",),
}
TILES = (8, 8, 8, 8, 8, 6, 8, 3)
LAST = (2, 0, 5, 5, 5, 2, 2, 0)
PRIORITY = (-3.8, 0.7, -15.5, -6.8, 3.8, -2.3, -0.6, -9.8, -0.1, -8.1, 10.2, 13.8, -22.0)
BACKLOG = 3.5
f32, bf16 = jnp.float32, jnp.bfloat16


def stage_bytes(width, last):
    first, cut = width - last, (last // LANES + 1) // 2 * LANES
    plane = lambda r, w: {d: r * w for d in range(4)}
    depth = lambda r, w: {d: r * w for d in (4, 5)}
    sizes = {
        "z0": depth(32, first), "s1": plane(64, first), "s2": plane(32, first),
        "s3a": plane(128, first), "s3b": plane(128, first), "s4": plane(128, first),
        "c1": plane(16, last), "c2": plane(16, cut), "c3": plane(64, last), "c4": plane(32, last),
        "c5a": depth(256, last), "c5b": depth(256, last), "c6": depth(256, last),
    }
    return {s: v for s, v in sizes.items() if sum(v.values()) > 0}


def arrange(chunks, work, latency=2.4, rate=46650.0):
    count, steps = len(chunks), list(NEEDS)
    sizes = [stage_bytes(width, last) for _, width, last in chunks]
    free, land, staged, ended = [0.0] * 6, {}, [None] * count, {}
    todo = [(k, s) for k in range(count) for s in sizes[k]]
    todo.sort(key=lambda c: (c[0] + PRIORITY[steps.index(c[1])], steps.index(c[1])))
    order, now, work, never = [], 0.0, list(work), 1e9
    whole = lambda k: max(land.get((k, s), never) for s in sizes[k])
    while todo or work:
        pick, later = None, never
        for k, s in todo:
            if staged[k] is None:
                continue
            ready = max(
                [staged[k]] + [land.get((k, d), never) for d in NEEDS[s] if d in sizes[k]]
            )
            queue = max(free[d] for d in sizes[k][s]) - now
            if ready > now:
                later = min(later, ready)
            elif queue > BACKLOG:
                later = min(later, now + queue - BACKLOG + 1e-6)
            else:
                pick = (k, s)
                break
        if pick:
            k, s = pick
            todo.remove(pick)
            order.append(pick)
            for d, size in sizes[k][s].items():
                free[d] = max(free[d], now) + size * 2 / rate
            land[pick] = max(free[d] for d in sizes[k][s]) + latency
            now += 0.15
            continue
        if work:
            name, cost, reads, after = work[0]
            ready = max(
                [0.0] + [whole(k) for k in reads] + [ended[w] + delay for w, delay in after]
            )
            if ready <= now:
                work.pop(0)
                order.append((-1, name))
                now += cost
                ended[name] = now
                if name[:5] == "stage":
                    staged[int(name[5:])] = now
                continue
            if ready < never:
                later = min(later, ready)
        now = later
    return order


WORK = (
    tuple((f"stage{k}", 0.4, (), ()) for k in range(len(TILES)))
    + (("prep", 1.0, (), ()), ("norm1", 1.5, (), ()), ("in", 3.8, (0,), ()))
    + tuple((f"scan{i}", 3.3, (), ()) for i in range(4))
    + (
        ("gate0", 2.4, (1,), ()), ("gate1", 2.4, (), ()), ("outA", 2.2, (2,), ()),
        ("outH", 2.2, (), ()), ("mixed", 1.0, (), (("outA", 3.0),)),
        ("norm2", 1.5, (), (("mixed", 3.2),)), ("hid0", 4.0, (3,), ()), ("hid1", 4.0, (4,), ()),
        ("hid2", 3.0, (5,), ()), ("downA", 2.5, (6,), ()), ("downH", 2.5, (), ()),
        ("last", 4.0, (7,), ()),
    )
)


def sigmoid(v):
    return 1.0 / (1.0 + jnp.exp(-v))


def layer_kernel(
    chunks, tok, w_in, w_gate, w_out, w_fg, w_fu, w_dn,
    mix_gain, in_scale, gt_scale, conv_ref, recur_ref, ingate_ref, decay_ref, extra_ref,
    out_scale, ffn_gain, fg_scale, fu_scale, dn_scale, out_ref,
    W, X, N, BI, ST, GA, SB, RB, RB2, H, PS, F1, F2, F3, F4, F5, F6, F7, F8, MAP, RATES, EX,
    send_sem, recv_sem, tp_send, tp_recv, own_sem,
):
    rep, fs, tp = lax.axis_index("rep"), lax.axis_index("fs"), lax.axis_index("tp")
    zl, y, x = fs // 16, (fs // 4) % 4, fs % 4
    rows, half = X.shape[1:]
    n = len(chunks)
    up = lambda v: lax.rem(v + 1, 4)
    dn = lambda v: lax.rem(v + 3, 4)
    xl, xr, yl, yr = dn(x), up(x), dn(y), up(y)
    other, away_zl = 1 - tp, 1 - zl
    to_x = lambda v: (rep, zl * 16 + y * 4 + v, tp)
    to_y = lambda v: (rep, zl * 16 + v * 4 + x, tp)
    z_other = away_zl * 16 + y * 4 + x
    rep_next = jnp.where(zl == 0, rep, 1 - rep)
    rep_prev = 1 - rep_next
    z_next, z_prev = (rep_next, z_other, tp), (rep_prev, z_other, tp)
    partner = (rep, fs, other)

    barrier = pltpu.get_barrier_semaphore()
    for peer in (to_x(xl), to_x(xr), to_y(yl), to_y(yr), z_next, z_prev, partner):
        pl.semaphore_signal(barrier, inc=1, device_id=peer, device_id_type=MESH)

    loads = []
    for i, (src, dst) in enumerate(
        [
            (w_in, F1), (tok, X.at[tp]), (w_gate, F2), (w_out, F3), (w_fg, F4), (w_fu, F5),
            (w_dn, F6), (recur_ref, F7), (ingate_ref, F8),
        ]
    ):
        c = pltpu.make_async_copy(src, dst, own_sem.at[i])
        c.start()
        loads.append(c)
    keep = loads.pop(1)

    def remote(src, dst, target, ssem, rsem):
        return pltpu.make_async_remote_copy(
            src_ref=src, dst_ref=dst, send_sem=ssem, recv_sem=rsem,
            device_id=target, device_id_type=MESH,
        )

    A, B = pl.ds(0, 32), pl.ds(32, 32)
    every = slice(None)
    lo2, hi2 = pl.ds(0, 2), pl.ds(2, 2)
    mine_rows = pl.ds(pl.multiple_of(rep * 32, 32), 32)
    CA = pl.ds(pl.multiple_of(rep * 32, 16), 16)
    CB = pl.ds(pl.multiple_of(rep * 32 + 16, 16), 16)
    next_rows = pl.ds(pl.multiple_of(rep_next * 32, 32), 32)
    prev_rows = pl.ds(pl.multiple_of(rep_prev * 32, 32), 32)
    up_x, dn_x, up_y, dn_y = to_x(xr), to_x(xl), to_y(yr), to_y(yl)
    def plan(k):
        start, width, last = chunks[k]
        cols, tail = pl.ds(start, width - last), pl.ds(start + width - last, last)
        cut = (last // LANES + 1) // 2 * LANES
        t1 = pl.ds(start + width - last, cut)
        t2 = pl.ds(start + width - last + cut, last - cut)
        at = lambda a, b, c, r: W.at[a, b, c, r, cols]
        ct = lambda a, b, c, r, t=tail: W.at[a, b, c, r, t] if t.size else None
        steps = {
            "z0": [(at(zl, y, x, A), z_next), (at(zl, y, x, B), z_prev)],
            "s1": [
                (at(every, y, x, A), up_x), (at(every, y, x, A), dn_x),
                (at(every, y, x, B), up_y), (at(every, y, x, B), dn_y),
            ],
            "s2": [
                (at(0, y, xl, A), up_x), (at(1, y, xr, A), dn_x),
                (at(0, yl, x, B), up_y), (at(1, yr, x, B), dn_y),
            ],
            "s3a": [
                (at(0, y, every, A), up_y), (at(1, y, every, A), dn_y),
                (at(0, every, x, B), up_x), (at(1, every, x, B), dn_x),
            ],
            "s3b": [
                (at(1, y, every, A), up_y), (at(0, y, every, A), dn_y),
                (at(1, every, x, B), up_x), (at(0, every, x, B), dn_x),
            ],
            "s4": [
                (at(0, yl, every, A), up_y), (at(1, yr, every, A), dn_y),
                (at(0, every, xl, B), up_x), (at(1, every, xr, B), dn_x),
            ],
            "c1": [
                (ct(zl, y, x, CA), up_x), (ct(zl, y, x, CA), dn_x),
                (ct(zl, y, x, CB), up_y), (ct(zl, y, x, CB), dn_y),
            ],
            "c2": [
                (ct(zl, y, xl, CA, t1), up_x), (ct(zl, y, xr, CA, t2), dn_x),
                (ct(zl, yl, x, CB, t1), up_y), (ct(zl, yr, x, CB, t2), dn_y),
            ],
            "c3": [
                (ct(zl, y, every, CA), up_y), (ct(zl, y, every, CA), dn_y),
                (ct(zl, every, x, CB), up_x), (ct(zl, every, x, CB), dn_x),
            ],
            "c4": [
                (ct(zl, yl, lo2, CA), up_y), (ct(zl, yr, hi2, CA), dn_y),
                (ct(zl, lo2, xl, CB), up_x), (ct(zl, hi2, xr, CB), dn_x),
            ],
            "c5a": [
                (ct(zl, lo2, every, mine_rows), z_next), (ct(zl, hi2, every, mine_rows), z_prev),
            ],
            "c5b": [
                (ct(zl, hi2, every, mine_rows), z_next), (ct(zl, lo2, every, mine_rows), z_prev),
            ],
            "c6": [
                (ct(away_zl, lo2, every, prev_rows), z_next),
                (ct(away_zl, hi2, every, next_rows), z_prev),
            ],
        }
        steps["c2"] = steps["c2"] if last > cut else steps["c2"][::2]
        sizes = stage_bytes(width, last)
        return {s: v for s, v in steps.items() if s in sizes}

    flights, landed = {}, set()

    def land(k, s):
        if (k, s) not in landed:
            landed.add((k, s))
            for c in flights[k, s]:
                c.wait_recv()

    def go(k, s):
        steps = plan(k)
        order = list(steps)
        for before in NEEDS[s]:
            if before in steps:
                land(k, before)
        base = sum(len(steps[o]) for o in order[: order.index(s)])
        flights[k, s] = []
        for i, (ref, target) in enumerate(steps[s]):
            c = remote(ref, ref, target, send_sem.at[k, base + i], recv_sem.at[k, base + i])
            c.start()
            flights[k, s].append(c)

    def done(k):
        for s in plan(k):
            land(k, s)

    def stage_weights(k):
        start = chunks[k][0]

        def put(at, value):
            W[zl, y, x, :, pl.ds(at, value.shape[1])] = value.astype(bf16)

        if k < 3:
            loads[k].wait()
            put(start, (F1, F2, F3)[k][...])
        elif k < 6:
            if k == 3:
                loads[3].wait()
                loads[4].wait()
            for t, unit in enumerate(units_of(k)):
                cut = slice(unit * LANES, (unit + 1) * LANES)
                put(start + t * 256, F4[:, cut])
                put(start + t * 256 + LANES, F5[:, cut])
        else:
            if k == 6:
                loads[5].wait()
            first = start - chunks[6][0]
            put(start, F6[:, first : first + chunks[k][1]])

    def units_of(k):
        first = (chunks[k][0] - chunks[3][0]) // 256
        return range(first, first + chunks[k][1] // 256)

    def prepare():
        zeros = jnp.zeros((64, 64), f32)
        loads[6].wait()
        loads[7].wait()
        for g in range(half // LANES):
            for p in range(2):
                r = F7[2 * g + p]
                q = F8[2 * g + p]
                parts = [r, zeros, q, zeros] if p == 0 else [zeros, r, zeros, q]
                MAP[g, p * 64 : p * 64 + 64, :] = jnp.concatenate(parts, axis=1)
        v = -decay_ref[...]
        RATES[...] = -RATE * (jnp.maximum(v, 0.0) + jnp.log1p(jnp.exp(-jnp.abs(v))))
        EX[...] = jnp.broadcast_to(extra_ref[...], (LANES, rows)).T

    def norm_rows(gain):
        step = 64

        def body(i, carry):
            r = pl.ds(pl.multiple_of(i * step, step), step)
            lo, hi = X[0, r, :].astype(f32), X[1, r, :].astype(f32)
            total = jnp.sum(lo * lo, axis=-1, keepdims=True) + jnp.sum(
                hi * hi, axis=-1, keepdims=True
            )
            scale = lax.rsqrt(total / (2 * half) + EPS)
            N[r, :half] = (lo * scale * gain[:, :half]).astype(bf16)
            N[r, half:] = (hi * scale * gain[:, half:]).astype(bf16)
            return carry

        lax.fori_loop(0, rows // step, body, 0)

    def wide(start, width):
        return W[:, :, :, :, pl.ds(start, width)].reshape(2 * half, width)

    def dot(a, b):
        return jnp.dot(a, b, preferred_element_type=f32)

    def dot_t(a, b):
        return lax.dot_general(a, b, (((1,), (1,)), ((), ())), preferred_element_type=f32)

    def branch_in():
        def body(i, carry):
            c = pl.multiple_of(i * 256, 256)
            BI[:, pl.ds(c, 256)] = (
                dot(N[...], wide(c, 256)) * in_scale[:, pl.ds(c, 256)]
            ).astype(bf16)
            return carry

        lax.fori_loop(0, half // 256, body, 0)

    def scan_block(i, carry):
        cols = pl.ds(pl.multiple_of(i * LANES, LANES), LANES)
        length = rows
        taps = conv_ref.shape[0]
        values = BI[:, cols].astype(f32)
        weights = conv_ref[:, cols]
        row = lax.broadcasted_iota(jnp.int32, values.shape, 0)
        conv = weights[taps - 1 : taps, :] * values
        for back in range(1, taps):
            moved = jnp.where(row >= back, pltpu.roll(values, back, 0), 0.0)
            conv = conv + weights[taps - 1 - back : taps - back, :] * moved
        mapped = jnp.dot(
            conv, MAP[i], preferred_element_type=f32, precision=lax.Precision.HIGHEST
        )
        recur = sigmoid(mapped[:, :LANES])
        ingate = sigmoid(mapped[:, LANES:])
        log_rate = RATES[:, cols] * recur - EX[...]
        a = jnp.exp(log_rate)
        u = -2.0 * log_rate
        series = u * (1 - u / 2 * (1 - u / 3 * (1 - u / 4 * (1 - u / 5 * (1 - u / 6)))))
        b = jnp.sqrt(jnp.where(u < 0.25, series, 1.0 - jnp.exp(-u))) * (ingate * conv)
        inner = row % 8
        for s in (1, 2, 4):
            live = inner >= s
            b = jnp.where(live, a * pltpu.roll(b, s, 0) + b, b)
            a = jnp.where(live, a * pltpu.roll(a, s, 0), a)
        groups = length // 8
        last_a = a.reshape(groups, 8, LANES)
        last_b = b.reshape(groups, 8, LANES)
        ca = jnp.broadcast_to(last_a[:, 7:8, :], last_a.shape).reshape(length, LANES)
        cb = jnp.broadcast_to(last_b[:, 7:8, :], last_b.shape).reshape(length, LANES)
        s = 8
        while s < length:
            cb_new = ca[s:] * cb[:-s] + cb[s:]
            ca_new = ca[s:] * ca[:-s]
            cb = jnp.concatenate([cb[:s], cb_new], axis=0)
            ca = jnp.concatenate([ca[:s], ca_new], axis=0)
            s *= 2
        ST[:, cols] = jnp.concatenate([b[:8], a[8:] * cb[:-8] + b[8:]], axis=0)
        return carry

    def gate_block(i, carry):
        c = pl.multiple_of(i * 256, 256)
        cols = pl.ds(c, 256)
        acc = dot(N[...], wide(pl.multiple_of(half + c, 256), 256)) * gt_scale[:, cols]
        g = acc.astype(bf16).astype(f32)
        gelu = 0.5 * g * (1.0 + jnp.tanh(0.7978845608028654 * (g + 0.044715 * g * g * g)))
        GA[:, cols] = (ST[:, cols] * gelu).astype(bf16)
        return carry

    def rows_of(block, j, start, width):
        return W[block, j, :, :, pl.ds(start, width)].reshape(256, width)

    own_cols = pl.ds(pl.multiple_of(tp * half, half), half)

    def out_away():
        def body(j, carry):
            cols = pl.ds(pl.multiple_of(j * 256, 256), 256)
            SB[:, cols] = dot_t(GA[...], rows_of(other, j, 2 * half, half)).astype(bf16)
            return carry

        lax.fori_loop(0, 4, body, 0)

    def out_home():
        def body(j, carry):
            cols = pl.ds(pl.multiple_of(j * 256, 256), 256)
            PS[0, :, cols] = dot_t(GA[...], rows_of(tp, j, 2 * half, half))
            return carry

        lax.fori_loop(0, 4, body, 0)

    def mix_rows():
        def body(i, carry):
            r = pl.ds(pl.multiple_of(i * 64, 64), 64)
            total = PS[0, r, :] + RB[r, :].astype(f32)
            X[tp, r, :] = (X[tp, r, :].astype(f32) + total * out_scale[:, own_cols]).astype(bf16)
            return carry

        lax.fori_loop(0, rows // 64, body, 0)

    def hidden_tile(unit, start):
        cols = pl.ds(pl.multiple_of(unit * LANES, LANES), LANES)
        both = dot(N[...], wide(start, 256))
        gate = both[:, :LANES] * fg_scale[cols].reshape(1, LANES)
        lift = both[:, LANES:] * fu_scale[cols].reshape(1, LANES)
        H[:, cols] = (gate / (1.0 + jnp.exp(-gate)) * lift).astype(bf16)

    def hidden(k):
        units, start = units_of(k), chunks[k][0]
        lax.fori_loop(
            0, len(units),
            lambda t, c: (
                hidden_tile(units[0] + t, pl.multiple_of(start + t * 256, 128)), c
            )[1], 0,
        )

    def down(k, block, j):
        start, width, _ = chunks[k]
        first = start - chunks[6][0]
        return dot_t(H[:, first : first + width], rows_of(block, j, start, width))

    def down_body(k, slot, block):
        def body(j, carry):
            cols = pl.ds(pl.multiple_of(j * 256, 256), 256)
            PS[slot, :, cols] = down(k, block, j)
            return carry

        lax.fori_loop(0, 4, body, 0)

    def finish(k):
        def away(j, carry):
            cols = pl.ds(pl.multiple_of(j * 256, 256), 256)
            SB[:, cols] = (PS[1, :, cols] + down(k, other, j)).astype(bf16)
            return carry

        def home(j, carry):
            c = pl.multiple_of(j * 256, 256)
            cols = pl.ds(c, 256)
            scale = dn_scale[:, pl.ds(pl.multiple_of(tp * half + c, 256), 256)]
            total = PS[0, :, cols] + down(k, tp, j) + RB2[:, cols].astype(f32)
            out_ref[:, cols] = (X[tp, :, cols].astype(f32) + total * scale).astype(bf16)
            return carry

        swaps = []
        for i in range(2):
            lax.fori_loop(2 * i, 2 * i + 2, away, 0)
            cols = pl.ds(i * (half // 2), half // 2)
            c = remote(SB.at[:, cols], RB2.at[:, cols], partner, tp_send.at[3 + i], tp_recv.at[3 + i])
            c.start()
            swaps.append(c)
        for i in range(2):
            swaps[i].wait_recv()
            lax.fori_loop(2 * i, 2 * i + 2, home, 0)
        for c in swaps:
            c.wait_send()

    swap_tok = remote(X.at[tp], X.at[tp], partner, tp_send.at[0], tp_recv.at[0])
    swap_out = remote(SB, RB, partner, tp_send.at[1], tp_recv.at[1])
    swap_mix = remote(X.at[tp], X.at[tp], partner, tp_send.at[2], tp_recv.at[2])

    def compute(name):
        if name == "stage0":
            stage_weights(0)
            pl.semaphore_wait(barrier, 7)
        elif name[:5] == "stage":
            stage_weights(int(name[5:]))
            if name == "stage1":
                keep.wait()
                swap_tok.start()
        elif name == "prep":
            prepare()
        elif name == "norm1":
            swap_tok.wait()
            norm_rows(mix_gain)
        elif name == "in":
            done(0)
            branch_in()
        elif name[:4] == "scan":
            i = int(name[4:])
            lax.fori_loop(2 * i, 2 * i + 2, scan_block, 0)
        elif name[:4] == "gate":
            done(1)
            i = int(name[4:])
            lax.fori_loop(2 * i, 2 * i + 2, gate_block, 0)
        elif name == "outA":
            done(2)
            out_away()
            swap_out.start()
        elif name == "outH":
            out_home()
        elif name == "mixed":
            swap_out.wait()
            mix_rows()
            swap_mix.start()
        elif name == "norm2":
            swap_mix.wait()
            norm_rows(ffn_gain)
        elif name[:3] == "hid":
            k = 3 + int(name[3:])
            done(k)
            hidden(k)
        elif name == "downA":
            done(6)
            down_body(6, 1, other)
        elif name == "downH":
            down_body(6, 0, tp)
        else:
            done(7)
            finish(7)

    for k, name in arrange(chunks, WORK):
        if k < 0:
            compute(name)
        else:
            go(k, name)
    for group in flights.values():
        for c in group:
            c.wait_send()


def local(*args):
    (
        tokens, mix_gain, lru_input, lru_gate, lru_input_scale, lru_gate_scale, conv_weight,
        recur_gate, input_gate, decay_rate, extra_decay, lru_output, lru_output_scale, ffn_gain,
        ffn_gate, ffn_up, ffn_gate_scale, ffn_up_scale, ffn_down, ffn_down_scale,
    ) = args
    rows, half = tokens.shape
    units = ffn_gate.shape[1] // LANES
    chunks, width = [], 0
    for tiles, last in zip(TILES, LAST):
        chunks.append((width, tiles * LANES, last * LANES))
        width += tiles * LANES
    assert sum(TILES[:3]) * LANES == 3 * half and sum(TILES[3:6]) == 2 * units
    assert sum(TILES[6:]) == units
    n = len(chunks)
    row = lambda v: v[None, :]
    vmem = pl.BlockSpec(memory_space=pltpu.VMEM)
    hbm = pl.BlockSpec(memory_space=pl.ANY)
    return pl.pallas_call(
        functools.partial(layer_kernel, tuple(chunks)),
        out_shape=jax.ShapeDtypeStruct((rows, half), bf16),
        in_specs=[hbm] * 7 + [vmem] * 4 + [hbm] * 2 + [vmem] * 7,
        out_specs=vmem,
        scratch_shapes=[
            pltpu.VMEM((2, 4, 4, 64, width), bf16),
            pltpu.VMEM((2, rows, half), bf16),
            pltpu.VMEM((rows, 2 * half), bf16),
            pltpu.VMEM((rows, half), bf16),
            pltpu.VMEM((rows, half), f32),
            pltpu.VMEM((rows, half), bf16),
            pltpu.VMEM((rows, half), bf16),
            pltpu.VMEM((rows, half), bf16),
            pltpu.VMEM((rows, half), bf16),
            pltpu.VMEM((rows, units * LANES), bf16),
            pltpu.VMEM((2, rows, half), f32),
            pltpu.VMEM(lru_input.shape, f32),
            pltpu.VMEM(lru_gate.shape, f32),
            pltpu.VMEM(lru_output.shape[::-1], f32),
            pltpu.VMEM(ffn_gate.shape, f32),
            pltpu.VMEM(ffn_up.shape, f32),
            pltpu.VMEM(ffn_down.shape[::-1], f32),
            pltpu.VMEM(recur_gate.shape, f32),
            pltpu.VMEM(input_gate.shape, f32),
            pltpu.VMEM((half // LANES, LANES, 2 * LANES), f32),
            pltpu.VMEM((1, half), f32),
            pltpu.VMEM((rows, LANES), f32),
            pltpu.SemaphoreType.DMA((n, 44)),
            pltpu.SemaphoreType.DMA((n, 44)),
            pltpu.SemaphoreType.DMA((5,)),
            pltpu.SemaphoreType.DMA((5,)),
            pltpu.SemaphoreType.DMA((9,)),
        ],
        compiler_params=pltpu.CompilerParams(
            collective_id=0, has_side_effects=True, vmem_limit_bytes=67043328
        ),
        name="layer",
    )(
        tokens, lru_input, lru_gate, lru_output.T, ffn_gate, ffn_up, ffn_down.T, row(mix_gain),
        row(lru_input_scale), row(lru_gate_scale), conv_weight, recur_gate, input_gate,
        row(decay_rate), row(extra_decay), row(lru_output_scale), row(ffn_gain),
        ffn_gate_scale, ffn_up_scale, row(ffn_down_scale),
    )


def solution(mesh):
    in_specs = (
        P(("rep", "fs"), "tp"), P(), P("fs", "tp"), P("fs", "tp"), P("tp"), P("tp"),
        P(None, "tp"), P("tp", None, None), P("tp", None, None), P("tp"), P(("rep", "fs")),
        P("tp", "fs"), P(), P(), P("fs", "tp"), P("fs", "tp"), P("tp"), P("tp"), P("tp", "fs"),
        P(),
    )
    return jax.shard_map(
        local, mesh=mesh, in_specs=in_specs, out_specs=P(("rep", "fs"), "tp"), check_vma=False
    )
```

```python
import functools

import jax
import jax.numpy as jnp
from jax import lax
from jax.experimental import pallas as pl
from jax.experimental.pallas import tpu as pltpu
from jax.sharding import PartitionSpec as P

EPS = 1e-06
RATE = 8.0
LANES = 128
MESH = pl.DeviceIdType.MESH
NEEDS = {
    "z0": (), "s1": ("z0",), "s2": ("s1",), "s3a": ("s2",), "s3b": ("s2",), "s4": ("s3a",),
    "c1": (), "c2": ("c1",), "c3": ("c2",), "c4": ("c3",), "c5a": ("c4",), "c5b": ("c4",),
    "c6": ("c5a",),
}
TILES = (8, 8, 8, 8, 8, 6, 8, 3)
LAST = (3, 4, 7, 0, 4, 2, 1, 1)
PRIORITY = (12.9, 0.9, 3.5, -7.5, 10.2, 10.3, -10.0, 3.7, -5.9, 2.9, 3.5, 7.4, 7.5)
VMEM = 67043328
BACKLOG = 2.0
f32, bf16 = jnp.float32, jnp.bfloat16


def stage_bytes(width, last):
    first, cut = width - last, (last // LANES + 1) // 2 * LANES
    plane = lambda r, w: {d: r * w for d in range(4)}
    depth = lambda r, w: {d: r * w for d in (4, 5)}
    sizes = {
        "z0": depth(32, first), "s1": plane(64, first), "s2": plane(32, first),
        "s3a": plane(128, first), "s3b": plane(128, first), "s4": plane(128, first),
        "c1": plane(16, last), "c2": plane(16, cut), "c3": plane(64, last), "c4": plane(32, last),
        "c5a": depth(256, last), "c5b": depth(256, last), "c6": depth(256, last),
    }
    return {s: v for s, v in sizes.items() if sum(v.values()) > 0}


def arrange(chunks, work, latency=2.2, rate=46650.0):
    count, steps = len(chunks), list(NEEDS)
    sizes = [stage_bytes(width, last) for _, width, last in chunks]
    free, land, staged, ended = [0.0] * 6, {}, [None] * count, {}
    todo = [(k, s) for k in range(count) for s in sizes[k]]
    todo.sort(key=lambda c: (c[0] + PRIORITY[steps.index(c[1])], steps.index(c[1])))
    order, now, work, never = [], 0.0, list(work), 1e9
    whole = lambda k: max(land.get((k, s), never) for s in sizes[k])
    while todo or work:
        pick, later = None, never
        for k, s in todo:
            if staged[k] is None:
                continue
            ready = max(
                [staged[k]] + [land.get((k, d), never) for d in NEEDS[s] if d in sizes[k]]
            )
            queue = max(free[d] for d in sizes[k][s]) - now
            if ready > now:
                later = min(later, ready)
            elif queue > BACKLOG:
                later = min(later, now + queue - BACKLOG + 1e-6)
            else:
                pick = (k, s)
                break
        if pick:
            k, s = pick
            todo.remove(pick)
            order.append(pick)
            for d, size in sizes[k][s].items():
                free[d] = max(free[d], now) + size * 2 / rate
            land[pick] = max(free[d] for d in sizes[k][s]) + latency
            now += 0.15
            continue
        if work:
            name, cost, reads, after = work[0]
            ready = max(
                [0.0] + [whole(k) for k in reads] + [ended[w] + delay for w, delay in after]
            )
            if ready <= now:
                work.pop(0)
                order.append((-1, name))
                now += cost
                ended[name] = now
                if name[:5] == "stage":
                    staged[int(name[5:])] = now
                continue
            if ready < never:
                later = min(later, ready)
        now = later
    return order


WORK = (
    tuple((f"stage{k}", 0.35, (), ()) for k in range(len(TILES)))
    + (("prep", 1.0, (), ()), ("norm1", 1.1, (), ()), ("in", 2.8, (0,), ()))
    + tuple((f"scan{i}", 2.4, (), ()) for i in range(4))
    + (
        ("gate0", 1.7, (1,), ()), ("gate1", 1.7, (), ()), ("outA", 1.6, (2,), ()),
        ("outH", 1.6, (), ()), ("mixed", 0.8, (), (("outA", 3.0),)),
        ("norm2", 1.1, (), (("mixed", 3.2),)), ("hid0", 2.9, (3,), ()), ("hid1", 2.9, (4,), ()),
        ("hid2", 2.2, (5,), ()), ("downA", 1.8, (6,), ()), ("downH", 1.8, (), ()),
        ("last", 3.0, (7,), ()),
    )
)


def sigmoid(v):
    return 1.0 / (1.0 + jnp.exp(-v))


def layer_kernel(
    chunks, tok, w_in, w_gate, w_out, w_fg, w_fu, w_dn,
    recur_in, ingate_in, *rest,
):
    small, out_ref, scratch = rest[:11], rest[11], rest[12:]
    (
        W, X, N, BI, ST, GA, SB, RB, RB2, H, PS, F1, F2, F3, F4, F5, F6, F7, F8, MAP, RATES, EX,
    ) = scratch[:22]
    kept = scratch[22:33]
    (
        mix_gain, in_scale, gt_scale, conv_ref, decay_ref, extra_ref, out_scale, ffn_gain,
        fg_scale, fu_scale, dn_scale,
    ) = kept
    send_sem, recv_sem, tp_send, tp_recv, own_sem = scratch[33:]
    rep, fs, tp = lax.axis_index("rep"), lax.axis_index("fs"), lax.axis_index("tp")
    zl, y, x = fs // 16, (fs // 4) % 4, fs % 4
    rows, half = X.shape[1:]
    n = len(chunks)
    up = lambda v: lax.rem(v + 1, 4)
    dn = lambda v: lax.rem(v + 3, 4)
    xl, xr, yl, yr = dn(x), up(x), dn(y), up(y)
    other, away_zl = 1 - tp, 1 - zl
    to_x = lambda v: (rep, zl * 16 + y * 4 + v, tp)
    to_y = lambda v: (rep, zl * 16 + v * 4 + x, tp)
    z_other = away_zl * 16 + y * 4 + x
    rep_next = jnp.where(zl == 0, rep, 1 - rep)
    rep_prev = 1 - rep_next
    z_next, z_prev = (rep_next, z_other, tp), (rep_prev, z_other, tp)
    partner = (rep, fs, other)

    barrier = pltpu.get_barrier_semaphore()
    for peer in (to_x(xl), to_x(xr), to_y(yl), to_y(yr), z_next, z_prev, partner):
        pl.semaphore_signal(barrier, inc=1, device_id=peer, device_id_type=MESH)

    loads = []
    for i, (src, dst) in enumerate(
        [
            (w_in, F1), (tok, X.at[tp]), (w_gate, F2), (w_out, F3), (w_fg, F4), (w_fu, F5),
            (w_dn, F6), (recur_in, F7), (ingate_in, F8), *zip(small, kept),
        ]
    ):
        c = pltpu.make_async_copy(src, dst, own_sem.at[i])
        c.start()
        loads.append(c)
    keep = loads.pop(1)

    def remote(src, dst, target, ssem, rsem):
        return pltpu.make_async_remote_copy(
            src_ref=src, dst_ref=dst, send_sem=ssem, recv_sem=rsem,
            device_id=target, device_id_type=MESH,
        )

    A, B = pl.ds(0, 32), pl.ds(32, 32)
    every = slice(None)
    lo2, hi2 = pl.ds(0, 2), pl.ds(2, 2)
    mine_rows = pl.ds(pl.multiple_of(rep * 32, 32), 32)
    CA = pl.ds(pl.multiple_of(rep * 32, 16), 16)
    CB = pl.ds(pl.multiple_of(rep * 32 + 16, 16), 16)
    next_rows = pl.ds(pl.multiple_of(rep_next * 32, 32), 32)
    prev_rows = pl.ds(pl.multiple_of(rep_prev * 32, 32), 32)
    up_x, dn_x, up_y, dn_y = to_x(xr), to_x(xl), to_y(yr), to_y(yl)
    def plan(k):
        start, width, last = chunks[k]
        cols, tail = pl.ds(start, width - last), pl.ds(start + width - last, last)
        cut = (last // LANES + 1) // 2 * LANES
        t1 = pl.ds(start + width - last, cut)
        t2 = pl.ds(start + width - last + cut, last - cut)
        at = lambda a, b, c, r: W.at[a, b, c, r, cols]
        ct = lambda a, b, c, r, t=tail: W.at[a, b, c, r, t] if t.size else None
        steps = {
            "z0": [(at(zl, y, x, A), z_next), (at(zl, y, x, B), z_prev)],
            "s1": [
                (at(every, y, x, A), up_x), (at(every, y, x, A), dn_x),
                (at(every, y, x, B), up_y), (at(every, y, x, B), dn_y),
            ],
            "s2": [
                (at(0, y, xl, A), up_x), (at(1, y, xr, A), dn_x),
                (at(0, yl, x, B), up_y), (at(1, yr, x, B), dn_y),
            ],
            "s3a": [
                (at(0, y, every, A), up_y), (at(1, y, every, A), dn_y),
                (at(0, every, x, B), up_x), (at(1, every, x, B), dn_x),
            ],
            "s3b": [
                (at(1, y, every, A), up_y), (at(0, y, every, A), dn_y),
                (at(1, every, x, B), up_x), (at(0, every, x, B), dn_x),
            ],
            "s4": [
                (at(0, yl, every, A), up_y), (at(1, yr, every, A), dn_y),
                (at(0, every, xl, B), up_x), (at(1, every, xr, B), dn_x),
            ],
            "c1": [
                (ct(zl, y, x, CA), up_x), (ct(zl, y, x, CA), dn_x),
                (ct(zl, y, x, CB), up_y), (ct(zl, y, x, CB), dn_y),
            ],
            "c2": [
                (ct(zl, y, xl, CA, t1), up_x), (ct(zl, y, xr, CA, t2), dn_x),
                (ct(zl, yl, x, CB, t1), up_y), (ct(zl, yr, x, CB, t2), dn_y),
            ],
            "c3": [
                (ct(zl, y, every, CA), up_y), (ct(zl, y, every, CA), dn_y),
                (ct(zl, every, x, CB), up_x), (ct(zl, every, x, CB), dn_x),
            ],
            "c4": [
                (ct(zl, yl, lo2, CA), up_y), (ct(zl, yr, hi2, CA), dn_y),
                (ct(zl, lo2, xl, CB), up_x), (ct(zl, hi2, xr, CB), dn_x),
            ],
            "c5a": [
                (ct(zl, lo2, every, mine_rows), z_next), (ct(zl, hi2, every, mine_rows), z_prev),
            ],
            "c5b": [
                (ct(zl, hi2, every, mine_rows), z_next), (ct(zl, lo2, every, mine_rows), z_prev),
            ],
            "c6": [
                (ct(away_zl, lo2, every, prev_rows), z_next),
                (ct(away_zl, hi2, every, next_rows), z_prev),
            ],
        }
        steps["c2"] = steps["c2"] if last > cut else steps["c2"][::2]
        sizes = stage_bytes(width, last)
        return {s: v for s, v in steps.items() if s in sizes}

    issued, landed = set(), set()
    stages = list(NEEDS)
    rows_of_stage = dict(zip(stages, (64, 256, 128, 512, 512, 512, 64, 32, 256, 128, 512, 512, 512)))
    arrive = dict(zip(stages, (0, 1, 2, 3, 4, 4, 5, 6, 7, 8, 9, 10, 10)))
    depart = dict(zip(stages, (0, 1, 2, 3, 3, 4, 5, 6, 7, 8, 9, 9, 10)))

    def whole_of(k, members):
        start, width, last = chunks[k]
        tail = members[0][0] == "c"
        cols = pl.ds(start + width - last, last) if tail else pl.ds(start, width - last)
        ref = {
            32: (0, 0, 0, pl.ds(0, 32), cols), 64: (0, 0, 0, every, cols),
            128: (0, 0, lo2, every, cols), 256: (0, 0, every, every, cols),
            512: (0, lo2, every, every, cols), 1024: (0, every, every, every, cols),
        }[sum(rows_of_stage[m] for m in members)]
        return W.at[ref]

    def wait_group(k, groups, g, arriving):
        members = [m for m in stages if groups[m] == g and (k, m) in issued]
        if members and (k, g, arriving) not in landed:
            landed.add((k, g, arriving))
            ref = whole_of(k, members)
            c = remote(ref, ref, partner, send_sem.at[k, g], recv_sem.at[k, g])
            c.wait_recv() if arriving else c.wait_send()

    def go(k, s):
        for before in NEEDS[s]:
            wait_group(k, arrive, arrive[before], True)
        issued.add((k, s))
        for ref, target in plan(k)[s]:
            remote(
                ref, ref, target, send_sem.at[k, depart[s]], recv_sem.at[k, arrive[s]]
            ).start()

    def done(k):
        for g in range(11):
            wait_group(k, arrive, g, True)

    def stage_weights(k):
        start = chunks[k][0]

        def put(at, value):
            W[zl, y, x, :, pl.ds(at, value.shape[1])] = value.astype(bf16)

        if k < 3:
            loads[k].wait()
            put(start, (F1, F2, F3)[k][...])
        elif k < 6:
            if k == 3:
                loads[3].wait()
                loads[4].wait()
            for t, unit in enumerate(units_of(k)):
                cut = slice(unit * LANES, (unit + 1) * LANES)
                put(start + t * 256, F4[:, cut])
                put(start + t * 256 + LANES, F5[:, cut])
        else:
            if k == 6:
                loads[5].wait()
            first = start - chunks[6][0]
            put(start, F6[:, first : first + chunks[k][1]])

    def units_of(k):
        first = (chunks[k][0] - chunks[3][0]) // 256
        return range(first, first + chunks[k][1] // 256)

    def prepare():
        zeros = jnp.zeros((64, 64), f32)
        for c in loads[6:]:
            c.wait()
        for g in range(half // LANES):
            for p in range(2):
                r = F7[2 * g + p]
                q = F8[2 * g + p]
                parts = [r, zeros, q, zeros] if p == 0 else [zeros, r, zeros, q]
                MAP[g, p * 64 : p * 64 + 64, :] = jnp.concatenate(parts, axis=1)
        v = -decay_ref[...]
        RATES[...] = -RATE * (jnp.maximum(v, 0.0) + jnp.log1p(jnp.exp(-jnp.abs(v))))
        EX[...] = jnp.broadcast_to(extra_ref[...], (LANES, rows)).T

    def norm_rows(gain):
        step = 64

        def body(i, carry):
            r = pl.ds(pl.multiple_of(i * step, step), step)
            lo, hi = X[0, r, :].astype(f32), X[1, r, :].astype(f32)
            total = jnp.sum(lo * lo, axis=-1, keepdims=True) + jnp.sum(
                hi * hi, axis=-1, keepdims=True
            )
            scale = lax.rsqrt(total / (2 * half) + EPS)
            N[r, :half] = (lo * scale * gain[:, :half]).astype(bf16)
            N[r, half:] = (hi * scale * gain[:, half:]).astype(bf16)
            return carry

        lax.fori_loop(0, rows // step, body, 0)

    def wide(start, width):
        return W[:, :, :, :, pl.ds(start, width)].reshape(2 * half, width)

    def dot(a, b):
        return jnp.dot(a, b, preferred_element_type=f32)

    def dot_t(a, b):
        return lax.dot_general(a, b, (((1,), (1,)), ((), ())), preferred_element_type=f32)

    def branch_in():
        def body(i, carry):
            c = pl.multiple_of(i * 256, 256)
            BI[:, pl.ds(c, 256)] = (
                dot(N[...], wide(c, 256)) * in_scale[:, pl.ds(c, 256)]
            ).astype(bf16)
            return carry

        lax.fori_loop(0, half // 256, body, 0)

    def scan_block(i, carry):
        cols = pl.ds(pl.multiple_of(i * LANES, LANES), LANES)
        length = rows
        taps = conv_ref.shape[0]
        values = BI[:, cols].astype(f32)
        weights = conv_ref[:, cols]
        row = lax.broadcasted_iota(jnp.int32, values.shape, 0)
        conv = weights[taps - 1 : taps, :] * values
        for back in range(1, taps):
            moved = jnp.where(row >= back, pltpu.roll(values, back, 0), 0.0)
            conv = conv + weights[taps - 1 - back : taps - back, :] * moved
        mapped = jnp.dot(
            conv, MAP[i], preferred_element_type=f32, precision=lax.Precision.HIGHEST
        )
        recur = sigmoid(mapped[:, :LANES])
        ingate = sigmoid(mapped[:, LANES:])
        log_rate = RATES[:, cols] * recur - EX[...]
        a = jnp.exp(log_rate)
        u = -2.0 * log_rate
        series = u * (1 - u / 2 * (1 - u / 3 * (1 - u / 4 * (1 - u / 5 * (1 - u / 6)))))
        b = jnp.sqrt(jnp.where(u < 0.25, series, 1.0 - jnp.exp(-u))) * (ingate * conv)
        inner = row % 8
        for s in (1, 2, 4):
            live = inner >= s
            b = jnp.where(live, a * pltpu.roll(b, s, 0) + b, b)
            a = jnp.where(live, a * pltpu.roll(a, s, 0), a)
        groups = length // 8
        last_a = a.reshape(groups, 8, LANES)
        last_b = b.reshape(groups, 8, LANES)
        ca = jnp.broadcast_to(last_a[:, 7:8, :], last_a.shape).reshape(length, LANES)
        cb = jnp.broadcast_to(last_b[:, 7:8, :], last_b.shape).reshape(length, LANES)
        s = 8
        while s < length:
            cb_new = ca[s:] * cb[:-s] + cb[s:]
            ca_new = ca[s:] * ca[:-s]
            cb = jnp.concatenate([cb[:s], cb_new], axis=0)
            ca = jnp.concatenate([ca[:s], ca_new], axis=0)
            s *= 2
        ST[:, cols] = jnp.concatenate([b[:8], a[8:] * cb[:-8] + b[8:]], axis=0)
        return carry

    def gate_block(i, carry):
        c = pl.multiple_of(i * 256, 256)
        cols = pl.ds(c, 256)
        acc = dot(N[...], wide(pl.multiple_of(half + c, 256), 256)) * gt_scale[:, cols]
        g = acc.astype(bf16).astype(f32)
        gelu = 0.5 * g * (1.0 + jnp.tanh(0.7978845608028654 * (g + 0.044715 * g * g * g)))
        GA[:, cols] = (ST[:, cols] * gelu).astype(bf16)
        return carry

    def rows_of(block, j, start, width):
        return W[block, j, :, :, pl.ds(start, width)].reshape(256, width)

    own_cols = pl.ds(pl.multiple_of(tp * half, half), half)

    def out_away():
        def body(j, carry):
            cols = pl.ds(pl.multiple_of(j * 256, 256), 256)
            SB[:, cols] = dot_t(GA[...], rows_of(other, j, 2 * half, half)).astype(bf16)
            return carry

        lax.fori_loop(0, 4, body, 0)

    def out_home():
        def body(j, carry):
            cols = pl.ds(pl.multiple_of(j * 256, 256), 256)
            PS[0, :, cols] = dot_t(GA[...], rows_of(tp, j, 2 * half, half))
            return carry

        lax.fori_loop(0, 4, body, 0)

    def mix_rows():
        def body(i, carry):
            r = pl.ds(pl.multiple_of(i * 64, 64), 64)
            total = PS[0, r, :] + RB[r, :].astype(f32)
            X[tp, r, :] = (X[tp, r, :].astype(f32) + total * out_scale[:, own_cols]).astype(bf16)
            return carry

        lax.fori_loop(0, rows // 64, body, 0)

    def hidden_tile(unit, start):
        cols = pl.ds(pl.multiple_of(unit * LANES, LANES), LANES)
        both = dot(N[...], wide(start, 256))
        gate = both[:, :LANES] * fg_scale[cols].reshape(1, LANES)
        lift = both[:, LANES:] * fu_scale[cols].reshape(1, LANES)
        H[:, cols] = (gate / (1.0 + jnp.exp(-gate)) * lift).astype(bf16)

    def hidden(k):
        units, start = units_of(k), chunks[k][0]
        lax.fori_loop(
            0, len(units),
            lambda t, c: (
                hidden_tile(units[0] + t, pl.multiple_of(start + t * 256, 128)), c
            )[1], 0,
        )

    def down(k, block, j):
        start, width, _ = chunks[k]
        first = start - chunks[6][0]
        return dot_t(H[:, first : first + width], rows_of(block, j, start, width))

    def down_body(k, slot, block):
        def body(j, carry):
            cols = pl.ds(pl.multiple_of(j * 256, 256), 256)
            PS[slot, :, cols] = down(k, block, j)
            return carry

        lax.fori_loop(0, 4, body, 0)

    def finish(k):
        def away(j, carry):
            cols = pl.ds(pl.multiple_of(j * 256, 256), 256)
            SB[:, cols] = (PS[1, :, cols] + down(k, other, j)).astype(bf16)
            return carry

        def home(j, carry):
            c = pl.multiple_of(j * 256, 256)
            cols = pl.ds(c, 256)
            scale = dn_scale[:, pl.ds(pl.multiple_of(tp * half + c, 256), 256)]
            total = PS[0, :, cols] + down(k, tp, j) + RB2[:, cols].astype(f32)
            GA[:, cols] = (X[tp, :, cols].astype(f32) + total * scale).astype(bf16)
            return carry

        swaps, outs = [], []
        for i in range(2):
            lax.fori_loop(2 * i, 2 * i + 2, away, 0)
            cols = pl.ds(i * (half // 2), half // 2)
            c = remote(SB.at[:, cols], RB2.at[:, cols], partner, tp_send.at[3 + i], tp_recv.at[3 + i])
            c.start()
            swaps.append(c)
        for i in range(2):
            swaps[i].wait_recv()
            lax.fori_loop(2 * i, 2 * i + 2, home, 0)
            cols = pl.ds(i * (half // 2), half // 2)
            c = pltpu.make_async_copy(GA.at[:, cols], out_ref.at[:, cols], tp_recv.at[5 + i])
            c.start()
            outs.append(c)
        for c in outs:
            c.wait()
        for c in swaps:
            c.wait_send()

    swap_tok = remote(X.at[tp], X.at[tp], partner, tp_send.at[0], tp_recv.at[0])
    swap_out = remote(SB, RB, partner, tp_send.at[1], tp_recv.at[1])
    swap_mix = remote(X.at[tp], X.at[tp], partner, tp_send.at[2], tp_recv.at[2])

    def compute(name):
        if name == "stage0":
            stage_weights(0)
            pl.semaphore_wait(barrier, 7)
        elif name[:5] == "stage":
            stage_weights(int(name[5:]))
            if name == "stage1":
                keep.wait()
                swap_tok.start()
        elif name == "prep":
            prepare()
        elif name == "norm1":
            swap_tok.wait()
            norm_rows(mix_gain)
        elif name == "in":
            done(0)
            branch_in()
        elif name[:4] == "scan":
            i = int(name[4:])
            lax.fori_loop(2 * i, 2 * i + 2, scan_block, 0)
        elif name[:4] == "gate":
            done(1)
            i = int(name[4:])
            lax.fori_loop(2 * i, 2 * i + 2, gate_block, 0)
        elif name == "outA":
            done(2)
            out_away()
            swap_out.start()
        elif name == "outH":
            out_home()
        elif name == "mixed":
            swap_out.wait()
            mix_rows()
            swap_mix.start()
        elif name == "norm2":
            swap_mix.wait()
            norm_rows(ffn_gain)
        elif name[:3] == "hid":
            k = 3 + int(name[3:])
            done(k)
            hidden(k)
        elif name == "downA":
            done(6)
            down_body(6, 1, other)
        elif name == "downH":
            down_body(6, 0, tp)
        else:
            done(7)
            finish(7)

    for k, name in arrange(chunks, WORK):
        if k < 0:
            compute(name)
        else:
            go(k, name)
    for k in range(n):
        for g in range(11):
            wait_group(k, depart, g, False)


def local(*args):
    (
        tokens, mix_gain, lru_input, lru_gate, lru_input_scale, lru_gate_scale, conv_weight,
        recur_gate, input_gate, decay_rate, extra_decay, lru_output, lru_output_scale, ffn_gain,
        ffn_gate, ffn_up, ffn_gate_scale, ffn_up_scale, ffn_down, ffn_down_scale,
    ) = args
    rows, half = tokens.shape
    units = ffn_gate.shape[1] // LANES
    chunks, width = [], 0
    for tiles, last in zip(TILES, LAST):
        chunks.append((width, tiles * LANES, last * LANES))
        width += tiles * LANES
    assert sum(TILES[:3]) * LANES == 3 * half and sum(TILES[3:6]) == 2 * units
    assert sum(TILES[6:]) == units
    n = len(chunks)
    row = lambda v: v[None, :]
    small = (
        row(mix_gain), row(lru_input_scale), row(lru_gate_scale), conv_weight, row(decay_rate),
        row(extra_decay), row(lru_output_scale), row(ffn_gain), ffn_gate_scale, ffn_up_scale,
        row(ffn_down_scale),
    )
    hbm = pl.BlockSpec(memory_space=pl.ANY)
    return pl.pallas_call(
        functools.partial(layer_kernel, tuple(chunks)),
        out_shape=jax.ShapeDtypeStruct((rows, half), bf16),
        in_specs=[hbm] * 20,
        out_specs=hbm,
        scratch_shapes=[
            pltpu.VMEM((2, 4, 4, 64, width), bf16),
            pltpu.VMEM((2, rows, half), bf16),
            pltpu.VMEM((rows, 2 * half), bf16),
            pltpu.VMEM((rows, half), bf16),
            pltpu.VMEM((rows, half), f32),
            pltpu.VMEM((rows, half), bf16),
            pltpu.VMEM((rows, half), bf16),
            pltpu.VMEM((rows, half), bf16),
            pltpu.VMEM((rows, half), bf16),
            pltpu.VMEM((rows, units * LANES), bf16),
            pltpu.VMEM((2, rows, half), f32),
            pltpu.VMEM(lru_input.shape, f32),
            pltpu.VMEM(lru_gate.shape, f32),
            pltpu.VMEM(lru_output.shape[::-1], f32),
            pltpu.VMEM(ffn_gate.shape, f32),
            pltpu.VMEM(ffn_up.shape, f32),
            pltpu.VMEM(ffn_down.shape[::-1], f32),
            pltpu.VMEM(recur_gate.shape, f32),
            pltpu.VMEM(input_gate.shape, f32),
            pltpu.VMEM((half // LANES, LANES, 2 * LANES), f32),
            pltpu.VMEM((1, half), f32),
            pltpu.VMEM((rows, LANES), f32),
            *(pltpu.VMEM(v.shape, f32) for v in small),
            pltpu.SemaphoreType.DMA((n, 11)),
            pltpu.SemaphoreType.DMA((n, 11)),
            pltpu.SemaphoreType.DMA((5,)),
            pltpu.SemaphoreType.DMA((7,)),
            pltpu.SemaphoreType.DMA((20,)),
        ],
        compiler_params=pltpu.CompilerParams(
            collective_id=0, has_side_effects=True, vmem_limit_bytes=VMEM
        ),
        name="layer",
    )(
        tokens, lru_input, lru_gate, lru_output.T, ffn_gate, ffn_up, ffn_down.T, recur_gate,
        input_gate, *small,
    )


def solution(mesh):
    in_specs = (
        P(("rep", "fs"), "tp"), P(), P("fs", "tp"), P("fs", "tp"), P("tp"), P("tp"),
        P(None, "tp"), P("tp", None, None), P("tp", None, None), P("tp"), P(("rep", "fs")),
        P("tp", "fs"), P(), P(), P("fs", "tp"), P("fs", "tp"), P("tp"), P("tp"), P("tp", "fs"),
        P(),
    )
    return jax.shard_map(
        local, mesh=mesh, in_specs=in_specs, out_specs=P(("rep", "fs"), "tp"), check_vma=False
    )
```

```python
import functools

import jax
import jax.numpy as jnp
from jax import lax
from jax.experimental import pallas as pl
from jax.experimental.pallas import tpu as pltpu
from jax.sharding import PartitionSpec as P

EPS = 1e-06
RATE = 8.0
LANES = 128
MESH = pl.DeviceIdType.MESH
NEEDS = {
    "z0": (), "s1": ("z0",), "s2": ("s1",), "s3a": ("s2",), "s3b": ("s2",), "s4": ("s3a",),
    "c1": (), "c2": ("c1",), "c3": ("c2",), "c4": ("c3",), "c5a": ("c4",), "c5b": ("c4",),
    "c6": ("c5a",),
}
TILES = (8, 8, 8, 8, 8, 6, 8, 3)
LAST = (0, 0, 1, 6, 3, 2, 3, 1)
PRIORITY = (-7.1, -0.6, -10.7, 3.2, 3.9, -0.6, -8.8, -1.4, -4.4, -5.4, -2.1, -2.5, -3.7)
VMEM = 67043328
BACKLOG = 5.0
f32, bf16 = jnp.float32, jnp.bfloat16


def stage_bytes(width, last):
    first, cut = width - last, (last // LANES + 1) // 2 * LANES
    plane = lambda r, w: {d: r * w for d in range(4)}
    sizes = {
        "z0": {5: 64 * first}, "s1": plane(64, first), "s2": plane(32, first),
        "s3a": plane(128, first), "s3b": plane(128, first), "s4": plane(128, first),
        "c1": plane(16, last), "c2": plane(16, cut), "c3": plane(64, last), "c4": plane(32, last),
        "c5a": {4: 384 * last, 5: 128 * last}, "c5b": {4: 128 * last, 5: 384 * last},
        "c6": {4: 128 * last, 5: 384 * last},
    }
    return {s: v for s, v in sizes.items() if sum(v.values()) > 0}


def arrange(chunks, work, latency=2.2, rate=46650.0):
    count, steps = len(chunks), list(NEEDS)
    sizes = [stage_bytes(width, last) for _, width, last in chunks]
    free, land, staged, ended = [0.0] * 6, {}, [None] * count, {}
    todo = [(k, s) for k in range(count) for s in sizes[k]]
    todo.sort(key=lambda c: (c[0] + PRIORITY[steps.index(c[1])], steps.index(c[1])))
    todo = [(-2, i) for i in range(PIECES)] + todo
    order, now, work, never = [], 0.0, list(work), 1e9
    token_piece = {4: 512 * 1024 // PIECES}
    whole = lambda k: max(land.get((k, s), never) for s in sizes[k])
    while todo or work:
        pick, later = None, never
        for k, s in todo:
            if staged[max(k, 0)] is None:
                continue
            before = () if k < 0 else [d for d in NEEDS[s] if d in sizes[k]]
            ready = max([staged[max(k, 0)]] + [land.get((k, d), never) for d in before])
            queue = max(free[d] for d in (token_piece if k < 0 else sizes[k][s])) - now
            if ready > now:
                later = min(later, ready)
            elif queue > BACKLOG:
                later = min(later, now + queue - BACKLOG + 1e-6)
            else:
                pick = (k, s)
                break
        if pick:
            k, s = pick
            todo.remove(pick)
            order.append(pick)
            parts = token_piece if k < 0 else sizes[k][s]
            for d, size in parts.items():
                free[d] = max(free[d], now) + size * 2 / rate
            land[pick] = max(free[d] for d in parts) + latency
            if k < 0:
                ended["tokens"] = land[pick] if s == PIECES - 1 else never
            now += 0.15
            continue
        if work:
            name, cost, reads, after = work[0]
            ready = max(
                [0.0] + [whole(k) for k in reads] + [ended.get(w, never) + delay for w, delay in after]
            )
            if ready <= now:
                work.pop(0)
                order.append((-1, name))
                now += cost
                ended[name] = now
                if name[:5] == "stage":
                    staged[int(name[5:])] = now
                if name in SENDS:
                    free[4] = max(free[4], now) + SENDS[name] * 2 / rate
                    ended["sent" + name] = free[4] + latency
                continue
            if ready < never:
                later = min(later, ready)
        now = later
    return order


PIECES = 8
SENDS = {"gate0": 512 * 512}
WORK = (
    tuple((f"stage{k}", 0.35, (), ()) for k in range(len(TILES)))
    + (("prep", 1.0, (), ()), ("norm1", 1.1, (), ()),
       ("ptok", 0.2, (), (("tokens", 0.0),)), ("in1", 1.4, (0,), ()),
       ("norm1p", 1.1, (), (("ptok", 3.2),)), ("in0", 1.4, (), ()))
    + tuple((f"scan{i}", 2.4, (), ()) for i in range(4))
    + (
        ("gate0", 1.7, (1,), ()), ("gate1", 1.7, (), ()), ("outA", 1.6, (2,), (("sentgate0", 0.0),)),
        ("outH", 1.6, (), ()), ("mixed", 0.8, (), (("outA", 3.0),)),
        ("norm2", 1.1, (), (("mixed", 3.2),)), ("hid0", 2.9, (3,), ()), ("hid1", 2.9, (4,), ()),
        ("hid2", 2.2, (5,), ()), ("downA", 1.8, (6,), ()), ("downH", 1.8, (), ()),
        ("last", 3.0, (7,), ()),
    )
)


def sigmoid(v):
    return 1.0 / (1.0 + jnp.exp(-v))


def layer_kernel(
    chunks, tok, w_in, w_gate, w_out, w_fg, w_fu, w_dn,
    recur_in, ingate_in, *rest,
):
    small, out_ref, scratch = rest[:11], rest[11], rest[12:]
    (
        W, X, N, BI, ST, GA, SB, RB, RB2, H, PS, F1, F2, F3, F4, F5, F6, F7, F8, MAP, RATES, EX,
        XP, NP, GP, EP,
    ) = scratch[:26]
    kept = scratch[26:37]
    (
        mix_gain, in_scale, gt_scale, conv_ref, decay_ref, extra_ref, out_scale, ffn_gain,
        fg_scale, fu_scale, dn_scale,
    ) = kept
    send_sem, recv_sem, tp_send, tp_recv, own_sem = scratch[37:]
    rep, fs, tp = lax.axis_index("rep"), lax.axis_index("fs"), lax.axis_index("tp")
    zl, y, x = fs // 16, (fs // 4) % 4, fs % 4
    rows, half = X.shape[1:]
    n = len(chunks)
    up = lambda v: lax.rem(v + 1, 4)
    dn = lambda v: lax.rem(v + 3, 4)
    xl, xr, yl, yr = dn(x), up(x), dn(y), up(y)
    other, away_zl = 1 - tp, 1 - zl
    to_x = lambda v: (rep, zl * 16 + y * 4 + v, tp)
    to_y = lambda v: (rep, zl * 16 + v * 4 + x, tp)
    z_other = away_zl * 16 + y * 4 + x
    pair, apart = (rep, z_other, tp), (1 - rep, z_other, tp)
    partner = (rep, fs, other)

    barrier = pltpu.get_barrier_semaphore()
    for peer in (to_x(xl), to_x(xr), to_y(yl), to_y(yr), pair, apart, partner):
        pl.semaphore_signal(barrier, inc=1, device_id=peer, device_id_type=MESH)

    loads = []
    for i, (src, dst) in enumerate(
        [
            (w_in, F1), (tok, X.at[tp]), (w_gate, F2), (w_out, F3), (w_fg, F4), (w_fu, F5),
            (w_dn, F6), (recur_in, F7), (ingate_in, F8), *zip(small, kept),
        ]
    ):
        c = pltpu.make_async_copy(src, dst, own_sem.at[i])
        c.start()
        loads.append(c)
    keep = loads.pop(1)

    def remote(src, dst, target, ssem, rsem):
        return pltpu.make_async_remote_copy(
            src_ref=src, dst_ref=dst, send_sem=ssem, recv_sem=rsem,
            device_id=target, device_id_type=MESH,
        )

    A, B = pl.ds(0, 32), pl.ds(32, 32)
    every = slice(None)
    lo2, hi2 = pl.ds(0, 2), pl.ds(2, 2)
    mine_rows = pl.ds(pl.multiple_of(rep * 32, 32), 32)
    CA = pl.ds(pl.multiple_of(rep * 32, 16), 16)
    CB = pl.ds(pl.multiple_of(rep * 32 + 16, 16), 16)
    far_rows = pl.ds(pl.multiple_of((1 - rep) * 32, 32), 32)
    part = half // 2
    own_part, pair_part = pl.multiple_of(zl * part, part), pl.multiple_of(away_zl * part, part)
    up_x, dn_x, up_y, dn_y = to_x(xr), to_x(xl), to_y(yr), to_y(yl)
    def plan(k):
        start, width, last = chunks[k]
        cols, tail = pl.ds(start, width - last), pl.ds(start + width - last, last)
        cut = (last // LANES + 1) // 2 * LANES
        t1 = pl.ds(start + width - last, cut)
        t2 = pl.ds(start + width - last + cut, last - cut)
        if k < 2:
            cols = pl.ds(start + own_part, width)
        sent = pl.ds(start + pair_part, width) if k < 2 else cols
        at = lambda a, b, c, r: W.at[a, b, c, r, cols]
        ct = lambda a, b, c, r, t=tail: W.at[a, b, c, r, t] if t.size else None
        steps = {
            "z0": [(W.at[zl, y, x, :, sent], apart)],
            "s1": [
                (at(every, y, x, A), up_x), (at(every, y, x, A), dn_x),
                (at(every, y, x, B), up_y), (at(every, y, x, B), dn_y),
            ],
            "s2": [
                (at(0, y, xl, A), up_x), (at(1, y, xr, A), dn_x),
                (at(0, yl, x, B), up_y), (at(1, yr, x, B), dn_y),
            ],
            "s3a": [
                (at(0, y, every, A), up_y), (at(1, y, every, A), dn_y),
                (at(0, every, x, B), up_x), (at(1, every, x, B), dn_x),
            ],
            "s3b": [
                (at(1, y, every, A), up_y), (at(0, y, every, A), dn_y),
                (at(1, every, x, B), up_x), (at(0, every, x, B), dn_x),
            ],
            "s4": [
                (at(0, yl, every, A), up_y), (at(1, yr, every, A), dn_y),
                (at(0, every, xl, B), up_x), (at(1, every, xr, B), dn_x),
            ],
            "c1": [
                (ct(zl, y, x, CA), up_x), (ct(zl, y, x, CA), dn_x),
                (ct(zl, y, x, CB), up_y), (ct(zl, y, x, CB), dn_y),
            ],
            "c2": [
                (ct(zl, y, xl, CA, t1), up_x), (ct(zl, y, xr, CA, t2), dn_x),
                (ct(zl, yl, x, CB, t1), up_y), (ct(zl, yr, x, CB, t2), dn_y),
            ],
            "c3": [
                (ct(zl, y, every, CA), up_y), (ct(zl, y, every, CA), dn_y),
                (ct(zl, every, x, CB), up_x), (ct(zl, every, x, CB), dn_x),
            ],
            "c4": [
                (ct(zl, yl, lo2, CA), up_y), (ct(zl, yr, hi2, CA), dn_y),
                (ct(zl, lo2, xl, CB), up_x), (ct(zl, hi2, xr, CB), dn_x),
            ],
            "c5a": [
                *((ct(zl, j, every, mine_rows), pair) for j in (1, 2, 3)),
                (ct(zl, 0, every, mine_rows), apart),
            ],
            "c5b": [
                (ct(zl, 0, every, mine_rows), pair),
                *((ct(zl, j, every, mine_rows), apart) for j in (1, 2, 3)),
            ],
            "c6": [
                (ct(away_zl, 0, every, far_rows), pair),
                *((ct(away_zl, j, every, mine_rows), apart) for j in (1, 2, 3)),
            ],
        }
        steps["c2"] = steps["c2"] if last > cut else steps["c2"][::2]
        sizes = stage_bytes(width, last)
        return {s: v for s, v in steps.items() if s in sizes}

    issued, landed = set(), set()
    stages = list(NEEDS)
    rows_of_stage = dict(zip(stages, (64, 256, 128, 512, 512, 512, 64, 32, 256, 128, 512, 512, 512)))
    arrive = dict(zip(stages, (0, 1, 2, 3, 4, 4, 5, 6, 7, 8, 9, 10, 10)))
    depart = dict(zip(stages, (0, 1, 2, 3, 3, 4, 5, 6, 7, 8, 9, 9, 10)))

    def whole_of(k, members):
        start, width, last = chunks[k]
        tail = members[0][0] == "c"
        cols = pl.ds(start + width - last, last) if tail else pl.ds(start, width - last)
        ref = {
            32: (0, 0, 0, pl.ds(0, 32), cols), 64: (0, 0, 0, every, cols),
            128: (0, 0, lo2, every, cols), 256: (0, 0, every, every, cols),
            512: (0, lo2, every, every, cols), 1024: (0, every, every, every, cols),
        }[sum(rows_of_stage[m] for m in members)]
        return W.at[ref]

    def wait_group(k, groups, g, arriving):
        members = [m for m in stages if groups[m] == g and (k, m) in issued]
        if members and (k, g, arriving) not in landed:
            landed.add((k, g, arriving))
            ref = whole_of(k, members)
            c = remote(ref, ref, partner, send_sem.at[k, g], recv_sem.at[k, g])
            c.wait_recv() if arriving else c.wait_send()

    def go(k, s):
        for before in NEEDS[s]:
            wait_group(k, arrive, arrive[before], True)
        issued.add((k, s))
        for ref, target in plan(k)[s]:
            remote(
                ref, ref, target, send_sem.at[k, depart[s]], recv_sem.at[k, arrive[s]]
            ).start()

    def done(k):
        for g in range(11):
            wait_group(k, arrive, g, True)

    def stage_weights(k):
        start = chunks[k][0]

        def put(at, value):
            W[zl, y, x, :, pl.ds(at, value.shape[1])] = value.astype(bf16)

        if k < 3:
            loads[k].wait()
            put(start, (F1, F2, F3)[k][...])
        elif k < 6:
            if k == 3:
                loads[3].wait()
                loads[4].wait()
            for t, unit in enumerate(units_of(k)):
                cut = slice(unit * LANES, (unit + 1) * LANES)
                put(start + t * 256, F4[:, cut])
                put(start + t * 256 + LANES, F5[:, cut])
        else:
            if k == 6:
                loads[5].wait()
            first = start - chunks[6][0]
            put(start, F6[:, first : first + chunks[k][1]])

    def units_of(k):
        first = (chunks[k][0] - chunks[3][0]) // 256
        return range(first, first + chunks[k][1] // 256)

    def prepare():
        zeros = jnp.zeros((64, 64), f32)
        for c in loads[6:13] + loads[14:]:
            c.wait()
        for g in range(half // LANES):
            for p in range(2):
                r = F7[2 * g + p]
                q = F8[2 * g + p]
                parts = [r, zeros, q, zeros] if p == 0 else [zeros, r, zeros, q]
                MAP[g, p * 64 : p * 64 + 64, :] = jnp.concatenate(parts, axis=1)
        v = -decay_ref[...]
        RATES[...] = -RATE * (jnp.maximum(v, 0.0) + jnp.log1p(jnp.exp(-jnp.abs(v))))
        EX[1] = jnp.broadcast_to(extra_ref[...], (LANES, rows)).T

    def norm_rows(X, N, gain):
        step = 64

        def body(i, carry):
            r = pl.ds(pl.multiple_of(i * step, step), step)
            lo, hi = X[0, r, :].astype(f32), X[1, r, :].astype(f32)
            total = jnp.sum(lo * lo, axis=-1, keepdims=True) + jnp.sum(
                hi * hi, axis=-1, keepdims=True
            )
            scale = lax.rsqrt(total / (2 * half) + EPS)
            N[r, :half] = (lo * scale * gain[:, :half]).astype(bf16)
            N[r, half:] = (hi * scale * gain[:, half:]).astype(bf16)
            return carry

        lax.fori_loop(0, rows // step, body, 0)

    def wide(start, width):
        return W[:, :, :, :, pl.ds(start, width)].reshape(2 * half, width)

    def dot(a, b):
        return jnp.dot(a, b, preferred_element_type=f32)

    def dot_t(a, b):
        return lax.dot_general(a, b, (((1,), (1,)), ((), ())), preferred_element_type=f32)

    def branch_in(seq):
        def body(i, carry):
            c = pl.multiple_of(i * 256, 256)
            g = pl.multiple_of(own_part + c, 256)
            BI[seq, :, pl.ds(c, 256)] = (
                dot((NP, N)[seq][...], wide(g, 256)) * in_scale[:, pl.ds(g, 256)]
            ).astype(bf16)
            return carry

        lax.fori_loop(0, part // 256, body, 0)

    def scan_block(seq, i, carry):
        held = pl.ds(pl.multiple_of(i * LANES, LANES), LANES)
        cols = pl.ds(pl.multiple_of(own_part + i * LANES, LANES), LANES)
        length = rows
        taps = conv_ref.shape[0]
        values = BI[seq, :, held].astype(f32)
        weights = conv_ref[:, cols]
        row = lax.broadcasted_iota(jnp.int32, values.shape, 0)
        conv = weights[taps - 1 : taps, :] * values
        for back in range(1, taps):
            moved = jnp.where(row >= back, pltpu.roll(values, back, 0), 0.0)
            conv = conv + weights[taps - 1 - back : taps - back, :] * moved
        mapped = jnp.dot(
            conv, MAP[zl * (part // LANES) + i], preferred_element_type=f32, precision=lax.Precision.HIGHEST
        )
        recur = sigmoid(mapped[:, :LANES])
        ingate = sigmoid(mapped[:, LANES:])
        log_rate = RATES[:, cols] * recur - EX[seq]
        a = jnp.exp(log_rate)
        u = -2.0 * log_rate
        series = u * (1 - u / 2 * (1 - u / 3 * (1 - u / 4 * (1 - u / 5 * (1 - u / 6)))))
        b = jnp.sqrt(jnp.where(u < 0.25, series, 1.0 - jnp.exp(-u))) * (ingate * conv)
        inner = row % 8
        for s in (1, 2, 4):
            live = inner >= s
            b = jnp.where(live, a * pltpu.roll(b, s, 0) + b, b)
            a = jnp.where(live, a * pltpu.roll(a, s, 0), a)
        groups = length // 8
        last_a = a.reshape(groups, 8, LANES)
        last_b = b.reshape(groups, 8, LANES)
        ca = jnp.broadcast_to(last_a[:, 7:8, :], last_a.shape).reshape(length, LANES)
        cb = jnp.broadcast_to(last_b[:, 7:8, :], last_b.shape).reshape(length, LANES)
        s = 8
        while s < length:
            cb_new = ca[s:] * cb[:-s] + cb[s:]
            ca_new = ca[s:] * ca[:-s]
            cb = jnp.concatenate([cb[:s], cb_new], axis=0)
            ca = jnp.concatenate([ca[:s], ca_new], axis=0)
            s *= 2
        ST[seq, :, held] = jnp.concatenate([b[:8], a[8:] * cb[:-8] + b[8:]], axis=0)
        return carry

    def gate_block(seq, i, carry):
        c = pl.multiple_of(i * 256, 256)
        g = pl.multiple_of(own_part + c, 256)
        scale = gt_scale[:, pl.ds(g, 256)]
        acc = dot((NP, N)[seq][...], wide(pl.multiple_of(half + g, 256), 256)) * scale
        g16 = acc.astype(bf16).astype(f32)
        gelu = 0.5 * g16 * (
            1.0 + jnp.tanh(0.7978845608028654 * (g16 + 0.044715 * g16 * g16 * g16))
        )
        gated = (ST[seq, :, pl.ds(c, 256)] * gelu).astype(bf16)
        if seq == 0:
            GP[:, pl.ds(c, 256)] = gated
        else:
            GA[:, pl.ds(g, 256)] = gated
        return carry

    def rows_of(block, j, start, width):
        return W[block, j, :, :, pl.ds(start, width)].reshape(256, width)

    own_cols = pl.ds(pl.multiple_of(tp * half, half), half)

    def out_away():
        def body(j, carry):
            cols = pl.ds(pl.multiple_of(j * 256, 256), 256)
            SB[:, cols] = dot_t(GA[...], rows_of(other, j, 2 * half, half)).astype(bf16)
            return carry

        lax.fori_loop(0, 4, body, 0)

    def out_home():
        def body(j, carry):
            cols = pl.ds(pl.multiple_of(j * 256, 256), 256)
            PS[0, :, cols] = dot_t(GA[...], rows_of(tp, j, 2 * half, half))
            return carry

        lax.fori_loop(0, 4, body, 0)

    def mix_rows():
        def body(i, carry):
            r = pl.ds(pl.multiple_of(i * 64, 64), 64)
            total = PS[0, r, :] + RB[r, :].astype(f32)
            X[tp, r, :] = (X[tp, r, :].astype(f32) + total * out_scale[:, own_cols]).astype(bf16)
            return carry

        lax.fori_loop(0, rows // 64, body, 0)

    def hidden_tile(unit, start):
        cols = pl.ds(pl.multiple_of(unit * LANES, LANES), LANES)
        both = dot(N[...], wide(start, 256))
        gate = both[:, :LANES] * fg_scale[cols].reshape(1, LANES)
        lift = both[:, LANES:] * fu_scale[cols].reshape(1, LANES)
        H[:, cols] = (gate / (1.0 + jnp.exp(-gate)) * lift).astype(bf16)

    def hidden(k):
        units, start = units_of(k), chunks[k][0]
        lax.fori_loop(
            0, len(units),
            lambda t, c: (
                hidden_tile(units[0] + t, pl.multiple_of(start + t * 256, 128)), c
            )[1], 0,
        )

    def down(k, block, j):
        start, width, _ = chunks[k]
        first = start - chunks[6][0]
        return dot_t(H[:, first : first + width], rows_of(block, j, start, width))

    def down_body(k, slot, block):
        def body(j, carry):
            cols = pl.ds(pl.multiple_of(j * 256, 256), 256)
            PS[slot, :, cols] = down(k, block, j)
            return carry

        lax.fori_loop(0, 4, body, 0)

    def finish(k):
        def away(j, carry):
            cols = pl.ds(pl.multiple_of(j * 256, 256), 256)
            SB[:, cols] = (PS[1, :, cols] + down(k, other, j)).astype(bf16)
            return carry

        def home(j, carry):
            c = pl.multiple_of(j * 256, 256)
            cols = pl.ds(c, 256)
            scale = dn_scale[:, pl.ds(pl.multiple_of(tp * half + c, 256), 256)]
            total = PS[0, :, cols] + down(k, tp, j) + RB2[:, cols].astype(f32)
            GA[:, cols] = (X[tp, :, cols].astype(f32) + total * scale).astype(bf16)
            return carry

        swaps, outs = [], []
        for i in range(2):
            lax.fori_loop(2 * i, 2 * i + 2, away, 0)
            cols = pl.ds(i * (half // 2), half // 2)
            c = remote(SB.at[:, cols], RB2.at[:, cols], partner, tp_send.at[3 + i], tp_recv.at[3 + i])
            c.start()
            swaps.append(c)
        for i in range(2):
            swaps[i].wait_recv()
            lax.fori_loop(2 * i, 2 * i + 2, home, 0)
            cols = pl.ds(i * (half // 2), half // 2)
            c = pltpu.make_async_copy(GA.at[:, cols], out_ref.at[:, cols], tp_recv.at[5 + i])
            c.start()
            outs.append(c)
        for c in outs:
            c.wait()
        for c in swaps:
            c.wait_send()

    swap_tok = remote(X.at[tp], X.at[tp], partner, tp_send.at[0], tp_recv.at[0])
    swap_pair = remote(X.at[tp], XP.at[tp], pair, tp_send.at[5], tp_recv.at[7])
    swap_ptok = remote(XP.at[tp], XP.at[tp], partner, tp_send.at[6], tp_recv.at[8])
    swap_extra = remote(extra_ref, EP, pair, tp_send.at[7], tp_recv.at[9])
    swap_gated = remote(
        GP, GA.at[:, pl.ds(own_part, part)], pair, tp_send.at[8], tp_recv.at[10]
    )
    swap_out = remote(SB, RB, partner, tp_send.at[1], tp_recv.at[1])
    swap_mix = remote(X.at[tp], X.at[tp], partner, tp_send.at[2], tp_recv.at[2])

    def compute(name):
        if name == "stage0":
            stage_weights(0)
            pl.semaphore_wait(barrier, 7)
            loads[13].wait()
            swap_extra.start()
            keep.wait()
            swap_tok.start()
        elif name[:5] == "stage":
            stage_weights(int(name[5:]))
        elif name == "prep":
            prepare()
        elif name == "norm1":
            swap_tok.wait()
            norm_rows(X, N, mix_gain)
        elif name == "ptok":
            swap_pair.wait()
            swap_ptok.start()
        elif name == "norm1p":
            swap_ptok.wait()
            swap_extra.wait()
            EX[0] = jnp.broadcast_to(EP[...], (LANES, rows)).T
            norm_rows(XP, NP, mix_gain)
        elif name[:2] == "in":
            done(0)
            branch_in(int(name[2:]))
        elif name[:4] == "scan":
            i = int(name[4:])
            first = 2 * (i % 2)
            scan = functools.partial(scan_block, i // 2)
            lax.fori_loop(first, first + 2, scan, 0)
        elif name[:4] == "gate":
            done(1)
            i = int(name[4:])
            lax.fori_loop(0, 2, functools.partial(gate_block, i), 0)
            if i == 0:
                swap_gated.start()
        elif name == "outA":
            done(2)
            swap_gated.wait()
            out_away()
            swap_out.start()
        elif name == "outH":
            out_home()
        elif name == "mixed":
            swap_out.wait()
            mix_rows()
            swap_mix.start()
        elif name == "norm2":
            swap_mix.wait()
            norm_rows(X, N, ffn_gain)
        elif name[:3] == "hid":
            k = 3 + int(name[3:])
            done(k)
            hidden(k)
        elif name == "downA":
            done(6)
            down_body(6, 1, other)
        elif name == "downH":
            down_body(6, 0, tp)
        else:
            done(7)
            finish(7)

    for k, name in arrange(chunks, WORK):
        if k == -2:
            part_rows = pl.ds(name * (rows // PIECES), rows // PIECES)
            remote(
                X.at[tp, part_rows], XP.at[tp, part_rows], pair, tp_send.at[5], tp_recv.at[7]
            ).start()
        elif k < 0:
            compute(name)
        else:
            go(k, name)
    for k in range(n):
        for g in range(11):
            wait_group(k, depart, g, False)


def local(*args):
    (
        tokens, mix_gain, lru_input, lru_gate, lru_input_scale, lru_gate_scale, conv_weight,
        recur_gate, input_gate, decay_rate, extra_decay, lru_output, lru_output_scale, ffn_gain,
        ffn_gate, ffn_up, ffn_gate_scale, ffn_up_scale, ffn_down, ffn_down_scale,
    ) = args
    rows, half = tokens.shape
    units = ffn_gate.shape[1] // LANES
    chunks, width = [], 0
    for k, (tiles, last) in enumerate(zip(TILES, LAST)):
        chunks.append((width, (tiles // 2 if k < 2 else tiles) * LANES, last * LANES))
        width += tiles * LANES
    assert sum(TILES[:3]) * LANES == 3 * half and sum(TILES[3:6]) == 2 * units
    assert sum(TILES[6:]) == units
    n = len(chunks)
    row = lambda v: v[None, :]
    small = (
        row(mix_gain), row(lru_input_scale), row(lru_gate_scale), conv_weight, row(decay_rate),
        row(extra_decay), row(lru_output_scale), row(ffn_gain), ffn_gate_scale, ffn_up_scale,
        row(ffn_down_scale),
    )
    hbm = pl.BlockSpec(memory_space=pl.ANY)
    return pl.pallas_call(
        functools.partial(layer_kernel, tuple(chunks)),
        out_shape=jax.ShapeDtypeStruct((rows, half), bf16),
        in_specs=[hbm] * 20,
        out_specs=hbm,
        scratch_shapes=[
            pltpu.VMEM((2, 4, 4, 64, width), bf16),
            pltpu.VMEM((2, rows, half), bf16),
            pltpu.VMEM((rows, 2 * half), bf16),
            pltpu.VMEM((2, rows, half // 2), bf16),
            pltpu.VMEM((2, rows, half // 2), f32),
            pltpu.VMEM((rows, half), bf16),
            pltpu.VMEM((rows, half), bf16),
            pltpu.VMEM((rows, half), bf16),
            pltpu.VMEM((rows, half), bf16),
            pltpu.VMEM((rows, units * LANES), bf16),
            pltpu.VMEM((2, rows, half), f32),
            pltpu.VMEM(lru_input.shape, f32),
            pltpu.VMEM(lru_gate.shape, f32),
            pltpu.VMEM(lru_output.shape[::-1], f32),
            pltpu.VMEM(ffn_gate.shape, f32),
            pltpu.VMEM(ffn_up.shape, f32),
            pltpu.VMEM(ffn_down.shape[::-1], f32),
            pltpu.VMEM(recur_gate.shape, f32),
            pltpu.VMEM(input_gate.shape, f32),
            pltpu.VMEM((half // LANES, LANES, 2 * LANES), f32),
            pltpu.VMEM((1, half), f32),
            pltpu.VMEM((2, rows, LANES), f32),
            pltpu.VMEM((2, rows, half), bf16),
            pltpu.VMEM((rows, 2 * half), bf16),
            pltpu.VMEM((rows, half // 2), bf16),
            pltpu.VMEM((1, rows), f32),
            *(pltpu.VMEM(v.shape, f32) for v in small),
            pltpu.SemaphoreType.DMA((n, 11)),
            pltpu.SemaphoreType.DMA((n, 11)),
            pltpu.SemaphoreType.DMA((9,)),
            pltpu.SemaphoreType.DMA((11,)),
            pltpu.SemaphoreType.DMA((20,)),
        ],
        compiler_params=pltpu.CompilerParams(
            collective_id=0, has_side_effects=True, vmem_limit_bytes=VMEM
        ),
        name="layer",
    )(
        tokens, lru_input, lru_gate, lru_output.T, ffn_gate, ffn_up, ffn_down.T, recur_gate,
        input_gate, *small,
    )


def solution(mesh):
    in_specs = (
        P(("rep", "fs"), "tp"), P(), P("fs", "tp"), P("fs", "tp"), P("tp"), P("tp"),
        P(None, "tp"), P("tp", None, None), P("tp", None, None), P("tp"), P(("rep", "fs")),
        P("tp", "fs"), P(), P(), P("fs", "tp"), P("fs", "tp"), P("tp"), P("tp"), P("tp", "fs"),
        P(),
    )
    return jax.shard_map(
        local, mesh=mesh, in_specs=in_specs, out_specs=P(("rep", "fs"), "tp"), check_vma=False
    )
```

```python
import functools

import jax
import jax.numpy as jnp
from jax import lax
from jax.experimental import pallas as pl
from jax.experimental.pallas import tpu as pltpu
from jax.sharding import PartitionSpec as P

EPS = 1e-06
RATE = 8.0
LANES = 128
MESH = pl.DeviceIdType.MESH
NEEDS = {
    "z0": (), "s1": ("z0",), "s2": ("s1",), "s3a": ("s2",), "s3b": ("s2",), "s4": ("s3a",),
    "c1": (), "c2": ("c1",), "c3": ("c2",), "c4": ("c3",), "c5a": ("c4",), "c5b": ("c4",),
    "c6": ("c5a",),
}
TILES = (8, 8, 8, 8, 8, 6, 8, 3)
LAST = (0, 0, 3, 6, 3, 2, 1, 1)
PRIORITY = (-1.7, 2.7, -0.4, 5.3, 7.4, -16.7, -1.9, -0.9, -5.2, -12.8, -7.4, -8.0, -17.8)
VMEM = 67043328
BACKLOG = 5
f32, bf16 = jnp.float32, jnp.bfloat16


def stage_bytes(width, last):
    first, cut = width - last, (last // LANES + 1) // 2 * LANES
    plane = lambda r, w: {d: r * w for d in range(4)}
    sizes = {
        "z0": {5: 64 * first}, "s1": plane(64, first), "s2": plane(32, first),
        "s3a": plane(128, first), "s3b": plane(128, first), "s4": plane(128, first),
        "c1": plane(16, last), "c2": plane(16, cut), "c3": plane(64, last), "c4": plane(32, last),
        "c5a": {4: 384 * last, 5: 128 * last}, "c5b": {4: 128 * last, 5: 384 * last},
        "c6": {4: 128 * last, 5: 384 * last},
    }
    return {s: v for s, v in sizes.items() if sum(v.values()) > 0}


def arrange(chunks, work, latency=2.2, rate=46650.0):
    count, steps = len(chunks), list(NEEDS)
    sizes = [stage_bytes(width, last) for _, width, last in chunks]
    free, land, staged, ended = [0.0] * 6, {}, [None] * count, {}
    todo = [(k, s) for k in range(count) for s in sizes[k]]
    todo.sort(key=lambda c: (c[0] + PRIORITY[steps.index(c[1])], steps.index(c[1])))
    todo = [(-2, i) for i in range(PIECES)] + todo
    order, now, work, never = [], 0.0, list(work), 1e9
    token_piece = {4: 512 * 1024 // PIECES}
    whole = lambda k: max(land.get((k, s), never) for s in sizes[k])
    while todo or work:
        pick, later = None, never
        for k, s in todo:
            if staged[max(k, 0)] is None:
                continue
            before = () if k < 0 else [d for d in NEEDS[s] if d in sizes[k]]
            ready = max([staged[max(k, 0)]] + [land.get((k, d), never) for d in before])
            queue = max(free[d] for d in (token_piece if k < 0 else sizes[k][s])) - now
            if ready > now:
                later = min(later, ready)
            elif queue > BACKLOG:
                later = min(later, now + queue - BACKLOG + 1e-6)
            else:
                pick = (k, s)
                break
        if pick:
            k, s = pick
            todo.remove(pick)
            order.append(pick)
            parts = token_piece if k < 0 else sizes[k][s]
            for d, size in parts.items():
                free[d] = max(free[d], now) + size * 2 / rate
            land[pick] = max(free[d] for d in parts) + latency
            if k < 0:
                ended["tokens"] = land[pick] if s == PIECES - 1 else never
            now += 0.15
            continue
        if work:
            name, cost, reads, after = work[0]
            ready = max(
                [0.0] + [whole(k) for k in reads] + [ended.get(w, never) + delay for w, delay in after]
            )
            if ready <= now:
                work.pop(0)
                order.append((-1, name))
                now += cost
                ended[name] = now
                if name[:5] == "stage":
                    staged[int(name[5:])] = now
                if name in SENDS:
                    free[4] = max(free[4], now) + SENDS[name] * 2 / rate
                    ended["sent" + name] = free[4] + latency
                continue
            if ready < never:
                later = min(later, ready)
        now = later
    return order


PIECES = 8
SENDS = {"gate0": 512 * 512}
WORK = (
    tuple((f"stage{k}", 0.35, (), ()) for k in range(len(TILES)))
    + (("prep", 1.0, (), ()), ("norm1", 1.1, (), ()),
       ("ptok", 0.2, (), (("tokens", 0.0),)), ("in1", 1.4, (0,), ()),
       ("norm1p", 1.1, (), (("ptok", 3.2),)), ("in0", 1.4, (), ()))
    + tuple((f"scan{i}", 2.4, (), ()) for i in range(4))
    + (
        ("gate0", 1.7, (1,), ()), ("gate1", 1.7, (), ()), ("outA", 1.6, (2,), (("sentgate0", 0.0),)),
        ("outH", 1.6, (), ()), ("mixed", 0.8, (), (("outA", 3.0),)),
        ("norm2", 1.1, (), (("mixed", 3.2),)), ("hid0", 2.9, (3,), ()), ("hid1", 2.9, (4,), ()),
        ("hid2", 2.2, (5,), ()), ("downA", 1.8, (6,), ()), ("downH", 1.8, (), ()),
        ("last", 3.0, (7,), ()),
    )
)


def sigmoid(v):
    return 1.0 / (1.0 + jnp.exp(-v))


def layer_kernel(
    chunks, tok, w_in, w_gate, w_out, w_fg, w_fu, w_dn,
    recur_in, ingate_in, *rest,
):
    small, out_ref, scratch = rest[:11], rest[11], rest[12:]
    (
        W, X, N, BI, ST, GA, SB, RB, RB2, H, PS, F1, F2, F3, F4, F5, F6, F7, F8, MAP, RATES, EX,
        XP, NP, GP, EP,
    ) = scratch[:26]
    kept = scratch[26:37]
    (
        mix_gain, in_scale, gt_scale, conv_ref, decay_ref, extra_ref, out_scale, ffn_gain,
        fg_scale, fu_scale, dn_scale,
    ) = kept
    send_sem, recv_sem, tp_send, tp_recv, own_sem = scratch[37:]
    rep, fs, tp = lax.axis_index("rep"), lax.axis_index("fs"), lax.axis_index("tp")
    zl, y, x = fs // 16, (fs // 4) % 4, fs % 4
    rows, half = X.shape[1:]
    n = len(chunks)
    up = lambda v: lax.rem(v + 1, 4)
    dn = lambda v: lax.rem(v + 3, 4)
    xl, xr, yl, yr = dn(x), up(x), dn(y), up(y)
    other, away_zl = 1 - tp, 1 - zl
    to_x = lambda v: (rep, zl * 16 + y * 4 + v, tp)
    to_y = lambda v: (rep, zl * 16 + v * 4 + x, tp)
    z_other = away_zl * 16 + y * 4 + x
    pair, apart = (rep, z_other, tp), (1 - rep, z_other, tp)
    partner = (rep, fs, other)

    barrier = pltpu.get_barrier_semaphore()
    for peer in (to_x(xl), to_x(xr), to_y(yl), to_y(yr), pair, apart, partner):
        pl.semaphore_signal(barrier, inc=1, device_id=peer, device_id_type=MESH)

    loads = []
    for i, (src, dst) in enumerate(
        [
            (w_in, F1), (tok, X.at[tp]), (w_gate, F2), (w_out, F3), (w_fg, F4), (w_fu, F5),
            (w_dn, F6), (recur_in, F7), (ingate_in, F8), *zip(small, kept),
        ]
    ):
        c = pltpu.make_async_copy(src, dst, own_sem.at[i])
        c.start()
        loads.append(c)
    keep = loads.pop(1)

    def remote(src, dst, target, ssem, rsem):
        return pltpu.make_async_remote_copy(
            src_ref=src, dst_ref=dst, send_sem=ssem, recv_sem=rsem,
            device_id=target, device_id_type=MESH,
        )

    A, B = pl.ds(0, 32), pl.ds(32, 32)
    every = slice(None)
    lo2, hi2 = pl.ds(0, 2), pl.ds(2, 2)
    mine_rows = pl.ds(pl.multiple_of(rep * 32, 32), 32)
    CA = pl.ds(pl.multiple_of(rep * 32, 16), 16)
    CB = pl.ds(pl.multiple_of(rep * 32 + 16, 16), 16)
    far_rows = pl.ds(pl.multiple_of((1 - rep) * 32, 32), 32)
    part = half // 2
    own_part, pair_part = pl.multiple_of(zl * part, part), pl.multiple_of(away_zl * part, part)
    up_x, dn_x, up_y, dn_y = to_x(xr), to_x(xl), to_y(yr), to_y(yl)
    def plan(k):
        start, width, last = chunks[k]
        cols, tail = pl.ds(start, width - last), pl.ds(start + width - last, last)
        cut = (last // LANES + 1) // 2 * LANES
        t1 = pl.ds(start + width - last, cut)
        t2 = pl.ds(start + width - last + cut, last - cut)
        if k < 2:
            cols = pl.ds(start + own_part, width)
        sent = pl.ds(start + pair_part, width) if k < 2 else cols
        at = lambda a, b, c, r: W.at[a, b, c, r, cols]
        ct = lambda a, b, c, r, t=tail: W.at[a, b, c, r, t] if t.size else None
        steps = {
            "z0": [(W.at[zl, y, x, :, sent], apart)],
            "s1": [
                (at(every, y, x, A), up_x), (at(every, y, x, A), dn_x),
                (at(every, y, x, B), up_y), (at(every, y, x, B), dn_y),
            ],
            "s2": [
                (at(0, y, xl, A), up_x), (at(1, y, xr, A), dn_x),
                (at(0, yl, x, B), up_y), (at(1, yr, x, B), dn_y),
            ],
            "s3a": [
                (at(0, y, every, A), up_y), (at(1, y, every, A), dn_y),
                (at(0, every, x, B), up_x), (at(1, every, x, B), dn_x),
            ],
            "s3b": [
                (at(1, y, every, A), up_y), (at(0, y, every, A), dn_y),
                (at(1, every, x, B), up_x), (at(0, every, x, B), dn_x),
            ],
            "s4": [
                (at(0, yl, every, A), up_y), (at(1, yr, every, A), dn_y),
                (at(0, every, xl, B), up_x), (at(1, every, xr, B), dn_x),
            ],
            "c1": [
                (ct(zl, y, x, CA), up_x), (ct(zl, y, x, CA), dn_x),
                (ct(zl, y, x, CB), up_y), (ct(zl, y, x, CB), dn_y),
            ],
            "c2": [
                (ct(zl, y, xl, CA, t1), up_x), (ct(zl, y, xr, CA, t2), dn_x),
                (ct(zl, yl, x, CB, t1), up_y), (ct(zl, yr, x, CB, t2), dn_y),
            ],
            "c3": [
                (ct(zl, y, every, CA), up_y), (ct(zl, y, every, CA), dn_y),
                (ct(zl, every, x, CB), up_x), (ct(zl, every, x, CB), dn_x),
            ],
            "c4": [
                (ct(zl, yl, lo2, CA), up_y), (ct(zl, yr, hi2, CA), dn_y),
                (ct(zl, lo2, xl, CB), up_x), (ct(zl, hi2, xr, CB), dn_x),
            ],
            "c5a": [
                *((ct(zl, j, every, mine_rows), pair) for j in (1, 2, 3)),
                (ct(zl, 0, every, mine_rows), apart),
            ],
            "c5b": [
                (ct(zl, 0, every, mine_rows), pair),
                *((ct(zl, j, every, mine_rows), apart) for j in (1, 2, 3)),
            ],
            "c6": [
                (ct(away_zl, 0, every, far_rows), pair),
                *((ct(away_zl, j, every, mine_rows), apart) for j in (1, 2, 3)),
            ],
        }
        steps["c2"] = steps["c2"] if last > cut else steps["c2"][::2]
        sizes = stage_bytes(width, last)
        return {s: v for s, v in steps.items() if s in sizes}

    issued, landed = set(), set()
    stages = list(NEEDS)
    rows_of_stage = dict(zip(stages, (64, 256, 128, 512, 512, 512, 64, 32, 256, 128, 512, 512, 512)))
    arrive = dict(zip(stages, (0, 1, 2, 3, 4, 4, 5, 6, 7, 8, 9, 10, 10)))
    depart = dict(zip(stages, (0, 1, 2, 3, 3, 4, 5, 6, 7, 8, 9, 9, 10)))

    def whole_of(k, members):
        start, width, last = chunks[k]
        tail = members[0][0] == "c"
        cols = pl.ds(start + width - last, last) if tail else pl.ds(start, width - last)
        ref = {
            32: (0, 0, 0, pl.ds(0, 32), cols), 64: (0, 0, 0, every, cols),
            128: (0, 0, lo2, every, cols), 256: (0, 0, every, every, cols),
            512: (0, lo2, every, every, cols), 1024: (0, every, every, every, cols),
        }[sum(rows_of_stage[m] for m in members)]
        return W.at[ref]

    def wait_group(k, groups, g, arriving):
        members = [m for m in stages if groups[m] == g and (k, m) in issued]
        if members and (k, g, arriving) not in landed:
            landed.add((k, g, arriving))
            ref = whole_of(k, members)
            c = remote(ref, ref, partner, send_sem.at[k, g], recv_sem.at[k, g])
            c.wait_recv() if arriving else c.wait_send()

    def go(k, s):
        for before in NEEDS[s]:
            wait_group(k, arrive, arrive[before], True)
        issued.add((k, s))
        for ref, target in plan(k)[s]:
            remote(
                ref, ref, target, send_sem.at[k, depart[s]], recv_sem.at[k, arrive[s]]
            ).start()

    def done(k):
        for g in range(11):
            wait_group(k, arrive, g, True)

    def stage_weights(k):
        start = chunks[k][0]

        def put(at, value):
            W[zl, y, x, :, pl.ds(at, value.shape[1])] = value.astype(bf16)

        if k < 3:
            loads[k].wait()
            put(start, (F1, F2, F3)[k][...])
        elif k < 6:
            if k == 3:
                loads[3].wait()
                loads[4].wait()
            for t, unit in enumerate(units_of(k)):
                cut = slice(unit * LANES, (unit + 1) * LANES)
                put(start + t * 256, F4[:, cut])
                put(start + t * 256 + LANES, F5[:, cut])
        else:
            if k == 6:
                loads[5].wait()
            first = start - chunks[6][0]
            put(start, F6[:, first : first + chunks[k][1]])

    def units_of(k):
        first = (chunks[k][0] - chunks[3][0]) // 256
        return range(first, first + chunks[k][1] // 256)

    def prepare():
        zeros = jnp.zeros((64, 64), f32)
        for c in loads[6:13] + loads[14:]:
            c.wait()
        for g in range(half // LANES):
            for p in range(2):
                r = F7[2 * g + p]
                q = F8[2 * g + p]
                parts = [r, zeros, q, zeros] if p == 0 else [zeros, r, zeros, q]
                MAP[g, p * 64 : p * 64 + 64, :] = jnp.concatenate(parts, axis=1)
        v = -decay_ref[...]
        RATES[...] = -RATE * (jnp.maximum(v, 0.0) + jnp.log1p(jnp.exp(-jnp.abs(v))))
        EX[1] = jnp.broadcast_to(extra_ref[...], (LANES, rows)).T

    def norm_rows(X, N, gain):
        step = 64

        def body(i, carry):
            r = pl.ds(pl.multiple_of(i * step, step), step)
            lo, hi = X[0, r, :].astype(f32), X[1, r, :].astype(f32)
            total = jnp.sum(lo * lo, axis=-1, keepdims=True) + jnp.sum(
                hi * hi, axis=-1, keepdims=True
            )
            scale = lax.rsqrt(total / (2 * half) + EPS)
            N[r, :half] = (lo * scale * gain[:, :half]).astype(bf16)
            N[r, half:] = (hi * scale * gain[:, half:]).astype(bf16)
            return carry

        lax.fori_loop(0, rows // step, body, 0)

    def wide(start, width):
        return W[:, :, :, :, pl.ds(start, width)].reshape(2 * half, width)

    def dot(a, b):
        return jnp.dot(a, b, preferred_element_type=f32)

    def dot_t(a, b):
        return lax.dot_general(a, b, (((1,), (1,)), ((), ())), preferred_element_type=f32)

    def branch_in(seq):
        def body(i, carry):
            c = pl.multiple_of(i * 256, 256)
            g = pl.multiple_of(own_part + c, 256)
            BI[seq, :, pl.ds(c, 256)] = (
                dot((NP, N)[seq][...], wide(g, 256)) * in_scale[:, pl.ds(g, 256)]
            ).astype(bf16)
            return carry

        lax.fori_loop(0, part // 256, body, 0)

    def scan_block(seq, i, carry):
        held = pl.ds(pl.multiple_of(i * LANES, LANES), LANES)
        cols = pl.ds(pl.multiple_of(own_part + i * LANES, LANES), LANES)
        length = rows
        taps = conv_ref.shape[0]
        values = BI[seq, :, held].astype(f32)
        weights = conv_ref[:, cols]
        row = lax.broadcasted_iota(jnp.int32, values.shape, 0)
        conv = weights[taps - 1 : taps, :] * values
        for back in range(1, taps):
            moved = jnp.where(row >= back, pltpu.roll(values, back, 0), 0.0)
            conv = conv + weights[taps - 1 - back : taps - back, :] * moved
        mapped = jnp.dot(
            conv, MAP[zl * (part // LANES) + i], preferred_element_type=f32, precision=lax.Precision.HIGHEST
        )
        recur = sigmoid(mapped[:, :LANES])
        ingate = sigmoid(mapped[:, LANES:])
        log_rate = RATES[:, cols] * recur - EX[seq]
        a = jnp.exp(log_rate)
        u = -2.0 * log_rate
        series = u * (1 - u / 2 * (1 - u / 3 * (1 - u / 4 * (1 - u / 5 * (1 - u / 6)))))
        b = jnp.sqrt(jnp.where(u < 0.25, series, 1.0 - jnp.exp(-u))) * (ingate * conv)
        inner = row % 8
        for s in (1, 2, 4):
            live = inner >= s
            b = jnp.where(live, a * pltpu.roll(b, s, 0) + b, b)
            a = jnp.where(live, a * pltpu.roll(a, s, 0), a)
        groups = length // 8
        last_a = a.reshape(groups, 8, LANES)
        last_b = b.reshape(groups, 8, LANES)
        ca = jnp.broadcast_to(last_a[:, 7:8, :], last_a.shape).reshape(length, LANES)
        cb = jnp.broadcast_to(last_b[:, 7:8, :], last_b.shape).reshape(length, LANES)
        s = 8
        while s < length:
            cb_new = ca[s:] * cb[:-s] + cb[s:]
            ca_new = ca[s:] * ca[:-s]
            cb = jnp.concatenate([cb[:s], cb_new], axis=0)
            ca = jnp.concatenate([ca[:s], ca_new], axis=0)
            s *= 2
        ST[seq, :, held] = jnp.concatenate([b[:8], a[8:] * cb[:-8] + b[8:]], axis=0)
        return carry

    def gate_block(seq, i, carry):
        c = pl.multiple_of(i * 256, 256)
        g = pl.multiple_of(own_part + c, 256)
        scale = gt_scale[:, pl.ds(g, 256)]
        acc = dot((NP, N)[seq][...], wide(pl.multiple_of(half + g, 256), 256)) * scale
        g16 = acc.astype(bf16).astype(f32)
        gelu = 0.5 * g16 * (
            1.0 + jnp.tanh(0.7978845608028654 * (g16 + 0.044715 * g16 * g16 * g16))
        )
        gated = (ST[seq, :, pl.ds(c, 256)] * gelu).astype(bf16)
        if seq == 0:
            GP[:, pl.ds(c, 256)] = gated
        else:
            GA[:, pl.ds(g, 256)] = gated
        return carry

    def rows_of(block, j, start, width):
        return W[block, j, :, :, pl.ds(start, width)].reshape(256, width)

    own_cols = pl.ds(pl.multiple_of(tp * half, half), half)

    def out_away():
        def body(j, carry):
            cols = pl.ds(pl.multiple_of(j * 256, 256), 256)
            SB[:, cols] = dot_t(GA[...], rows_of(other, j, 2 * half, half)).astype(bf16)
            return carry

        lax.fori_loop(0, 4, body, 0)

    def out_home():
        def body(j, carry):
            cols = pl.ds(pl.multiple_of(j * 256, 256), 256)
            PS[0, :, cols] = dot_t(GA[...], rows_of(tp, j, 2 * half, half))
            return carry

        lax.fori_loop(0, 4, body, 0)

    def mix_rows():
        def body(i, carry):
            r = pl.ds(pl.multiple_of(i * 64, 64), 64)
            total = PS[0, r, :] + RB[r, :].astype(f32)
            X[tp, r, :] = (X[tp, r, :].astype(f32) + total * out_scale[:, own_cols]).astype(bf16)
            return carry

        lax.fori_loop(0, rows // 64, body, 0)

    def hidden_tile(unit, start):
        cols = pl.ds(pl.multiple_of(unit * LANES, LANES), LANES)
        both = dot(N[...], wide(start, 256))
        gate = both[:, :LANES] * fg_scale[cols].reshape(1, LANES)
        lift = both[:, LANES:] * fu_scale[cols].reshape(1, LANES)
        H[:, cols] = (gate / (1.0 + jnp.exp(-gate)) * lift).astype(bf16)

    def hidden(k):
        units, start = units_of(k), chunks[k][0]
        lax.fori_loop(
            0, len(units),
            lambda t, c: (
                hidden_tile(units[0] + t, pl.multiple_of(start + t * 256, 128)), c
            )[1], 0,
        )

    def down(k, block, j):
        start, width, _ = chunks[k]
        first = start - chunks[6][0]
        return dot_t(H[:, first : first + width], rows_of(block, j, start, width))

    def down_body(k, slot, block):
        def body(j, carry):
            cols = pl.ds(pl.multiple_of(j * 256, 256), 256)
            PS[slot, :, cols] = down(k, block, j)
            return carry

        lax.fori_loop(0, 4, body, 0)

    def finish(k):
        def away(j, carry):
            cols = pl.ds(pl.multiple_of(j * 256, 256), 256)
            SB[:, cols] = (PS[1, :, cols] + down(k, other, j)).astype(bf16)
            return carry

        def home(j, carry):
            c = pl.multiple_of(j * 256, 256)
            cols = pl.ds(c, 256)
            scale = dn_scale[:, pl.ds(pl.multiple_of(tp * half + c, 256), 256)]
            total = PS[0, :, cols] + down(k, tp, j) + RB2[:, cols].astype(f32)
            GA[:, cols] = (X[tp, :, cols].astype(f32) + total * scale).astype(bf16)
            return carry

        swaps, outs = [], []
        for i in range(2):
            lax.fori_loop(2 * i, 2 * i + 2, away, 0)
            cols = pl.ds(i * (half // 2), half // 2)
            c = remote(SB.at[:, cols], RB2.at[:, cols], partner, tp_send.at[3 + i], tp_recv.at[3 + i])
            c.start()
            swaps.append(c)
        for i in range(2):
            swaps[i].wait_recv()
            lax.fori_loop(2 * i, 2 * i + 2, home, 0)
            cols = pl.ds(i * (half // 2), half // 2)
            c = pltpu.make_async_copy(GA.at[:, cols], out_ref.at[:, cols], tp_recv.at[5 + i])
            c.start()
            outs.append(c)
        for c in outs:
            c.wait()
        for c in swaps:
            c.wait_send()

    swap_tok = remote(X.at[tp], X.at[tp], partner, tp_send.at[0], tp_recv.at[0])
    swap_pair = remote(X.at[tp], XP.at[tp], pair, tp_send.at[5], tp_recv.at[7])
    swap_ptok = remote(XP.at[tp], XP.at[tp], partner, tp_send.at[6], tp_recv.at[8])
    swap_extra = remote(extra_ref, EP, pair, tp_send.at[7], tp_recv.at[9])
    swap_gated = remote(
        GP, GA.at[:, pl.ds(own_part, part)], pair, tp_send.at[8], tp_recv.at[10]
    )
    swap_out = remote(SB, RB, partner, tp_send.at[1], tp_recv.at[1])
    swap_mix = remote(X.at[tp], X.at[tp], partner, tp_send.at[2], tp_recv.at[2])

    def compute(name):
        if name == "stage0":
            stage_weights(0)
            pl.semaphore_wait(barrier, 7)
            loads[13].wait()
            swap_extra.start()
            keep.wait()
            swap_tok.start()
        elif name[:5] == "stage":
            stage_weights(int(name[5:]))
        elif name == "prep":
            prepare()
        elif name == "norm1":
            swap_tok.wait()
            norm_rows(X, N, mix_gain)
        elif name == "ptok":
            swap_pair.wait()
            swap_ptok.start()
        elif name == "norm1p":
            swap_ptok.wait()
            swap_extra.wait()
            EX[0] = jnp.broadcast_to(EP[...], (LANES, rows)).T
            norm_rows(XP, NP, mix_gain)
        elif name[:2] == "in":
            done(0)
            branch_in(int(name[2:]))
        elif name[:4] == "scan":
            i = int(name[4:])
            first = 2 * (i % 2)
            scan = functools.partial(scan_block, i // 2)
            lax.fori_loop(first, first + 2, scan, 0)
        elif name[:4] == "gate":
            done(1)
            i = int(name[4:])
            lax.fori_loop(0, 2, functools.partial(gate_block, i), 0)
            if i == 0:
                swap_gated.start()
        elif name == "outA":
            done(2)
            swap_gated.wait()
            out_away()
            swap_out.start()
        elif name == "outH":
            out_home()
        elif name == "mixed":
            swap_out.wait()
            mix_rows()
            swap_mix.start()
        elif name == "norm2":
            swap_mix.wait()
            norm_rows(X, N, ffn_gain)
        elif name[:3] == "hid":
            k = 3 + int(name[3:])
            done(k)
            hidden(k)
        elif name == "downA":
            done(6)
            down_body(6, 1, other)
        elif name == "downH":
            down_body(6, 0, tp)
        else:
            done(7)
            finish(7)

    for k, name in arrange(chunks, WORK):
        if k == -2:
            part_rows = pl.ds(name * (rows // PIECES), rows // PIECES)
            remote(
                X.at[tp, part_rows], XP.at[tp, part_rows], pair, tp_send.at[5], tp_recv.at[7]
            ).start()
        elif k < 0:
            compute(name)
        else:
            go(k, name)
    for k in range(n):
        for g in range(11):
            wait_group(k, depart, g, False)


def local(*args):
    (
        tokens, mix_gain, lru_input, lru_gate, lru_input_scale, lru_gate_scale, conv_weight,
        recur_gate, input_gate, decay_rate, extra_decay, lru_output, lru_output_scale, ffn_gain,
        ffn_gate, ffn_up, ffn_gate_scale, ffn_up_scale, ffn_down, ffn_down_scale,
    ) = args
    rows, half = tokens.shape
    units = ffn_gate.shape[1] // LANES
    chunks, width = [], 0
    for k, (tiles, last) in enumerate(zip(TILES, LAST)):
        chunks.append((width, (tiles // 2 if k < 2 else tiles) * LANES, last * LANES))
        width += tiles * LANES
    assert sum(TILES[:3]) * LANES == 3 * half and sum(TILES[3:6]) == 2 * units
    assert sum(TILES[6:]) == units
    n = len(chunks)
    row = lambda v: v[None, :]
    small = (
        row(mix_gain), row(lru_input_scale), row(lru_gate_scale), conv_weight, row(decay_rate),
        row(extra_decay), row(lru_output_scale), row(ffn_gain), ffn_gate_scale, ffn_up_scale,
        row(ffn_down_scale),
    )
    hbm = pl.BlockSpec(memory_space=pl.ANY)
    return pl.pallas_call(
        functools.partial(layer_kernel, tuple(chunks)),
        out_shape=jax.ShapeDtypeStruct((rows, half), bf16),
        in_specs=[hbm] * 20,
        out_specs=hbm,
        scratch_shapes=[
            pltpu.VMEM((2, 4, 4, 64, width), bf16),
            pltpu.VMEM((2, rows, half), bf16),
            pltpu.VMEM((rows, 2 * half), bf16),
            pltpu.VMEM((2, rows, half // 2), bf16),
            pltpu.VMEM((2, rows, half // 2), f32),
            pltpu.VMEM((rows, half), bf16),
            pltpu.VMEM((rows, half), bf16),
            pltpu.VMEM((rows, half), bf16),
            pltpu.VMEM((rows, half), bf16),
            pltpu.VMEM((rows, units * LANES), bf16),
            pltpu.VMEM((2, rows, half), f32),
            pltpu.VMEM(lru_input.shape, f32),
            pltpu.VMEM(lru_gate.shape, f32),
            pltpu.VMEM(lru_output.shape[::-1], f32),
            pltpu.VMEM(ffn_gate.shape, f32),
            pltpu.VMEM(ffn_up.shape, f32),
            pltpu.VMEM(ffn_down.shape[::-1], f32),
            pltpu.VMEM(recur_gate.shape, f32),
            pltpu.VMEM(input_gate.shape, f32),
            pltpu.VMEM((half // LANES, LANES, 2 * LANES), f32),
            pltpu.VMEM((1, half), f32),
            pltpu.VMEM((2, rows, LANES), f32),
            pltpu.VMEM((2, rows, half), bf16),
            pltpu.VMEM((rows, 2 * half), bf16),
            pltpu.VMEM((rows, half // 2), bf16),
            pltpu.VMEM((1, rows), f32),
            *(pltpu.VMEM(v.shape, f32) for v in small),
            pltpu.SemaphoreType.DMA((n, 11)),
            pltpu.SemaphoreType.DMA((n, 11)),
            pltpu.SemaphoreType.DMA((9,)),
            pltpu.SemaphoreType.DMA((11,)),
            pltpu.SemaphoreType.DMA((20,)),
        ],
        compiler_params=pltpu.CompilerParams(
            collective_id=0, has_side_effects=True, vmem_limit_bytes=VMEM
        ),
        name="layer",
    )(
        tokens, lru_input, lru_gate, lru_output.T, ffn_gate, ffn_up, ffn_down.T, recur_gate,
        input_gate, *small,
    )


def solution(mesh):
    in_specs = (
        P(("rep", "fs"), "tp"), P(), P("fs", "tp"), P("fs", "tp"), P("tp"), P("tp"),
        P(None, "tp"), P("tp", None, None), P("tp", None, None), P("tp"), P(("rep", "fs")),
        P("tp", "fs"), P(), P(), P("fs", "tp"), P("fs", "tp"), P("tp"), P("tp"), P("tp", "fs"),
        P(),
    )
    return jax.shard_map(
        local, mesh=mesh, in_specs=in_specs, out_specs=P(("rep", "fs"), "tp"), check_vma=False
    )
```
